32 devices in a mesh: sp: 8 (over z, x), tp: 4 (over y, core).
Axes of the slice: x: 2, y: 2, z: 4, core: 2. Of those that a mesh axis runs over, the one named last changes fastest.
Arguments:
- cotangent: bfloat16 [1536, 2048], P('sp'), may hold values from -8 to 8
- residual: bfloat16 [1536, 2048], P('sp'), may hold values from -6 to 6
- norm_gain: float32 [2048], replicated, may hold values from 0.1 to 1.9
- route_ids: int32 [1536, 2], P('sp'), may hold values from 0 to 7, all different within a row; in each aligned block of 192 rows (0 to 191, 192 to 383, ...) at most 96 rows name the same one
- route_weights: float32 [1536, 2], P('sp'), may hold values from 0.1 to 1
- expert_gate: bfloat16 [8, 2048, 1024], P('sp', None, 'tp'), may hold values from -0.125 to 0.125
- expert_up: bfloat16 [8, 2048, 1024], P('sp', None, 'tp'), may hold values from -0.125 to 0.125
- expert_down: bfloat16 [8, 1024, 2048], P('sp', 'tp'), may hold values from -0.1875 to 0.1875
- out_proj: bfloat16 [2048, 1024], P(None, 'tp'), may hold values from -0.1875 to 0.1875
- conv_out: bfloat16 [1536, 1024], P('sp', 'tp'), may hold values from -6 to 6, as said below
- branch_gate: bfloat16 [1536, 1024], P('sp', 'tp'), may hold values from -6 to 6
- prev_state: bfloat16 [1536, 1024], P('sp', 'tp'), may hold values from -6 to 6
- decay_param: float32 [1024], P('tp'), as said below
- rate_map: bfloat16 [16, 64, 64], P('tp'), may hold values from -0.75 to 0.75
- input_map: bfloat16 [16, 64, 64], P('tp'), may hold values from -0.75 to 0.75
Outputs:
- grad_gate: float32 [8, 2048, 1024], P('sp', None, 'tp')
- grad_up: float32 [8, 2048, 1024], P('sp', None, 'tp')
- grad_down: float32 [8, 1024, 2048], P('sp', 'tp')
- grad_out_proj: float32 [2048, 1024], P('sp', 'tp')
- grad_conv_out: float32 [1536, 1024], P('sp', 'tp')
- grad_branch_gate: float32 [1536, 1024], P('sp', 'tp')
The draws below stay inside these ranges and needn't reach their ends.
Inputs may be any that keep to these rules, and one draw needn't show every extreme that they name: `route_ids`: within the rows of one device (aligned blocks of 192 rows) no expert is named by more than 96 rows, a bound that some block reaches; the two ids of a row differ. `conv_out`: every entry is a finite value between -6 and 6. `decay_param`: every channel's decay parameter is at least 4.
All inputs are finite; a program needn't handle non-finite values.
Results may differ from the reference program's by a relative error of at most 0.0095.
Values may be sent and summed in bfloat16 or wider, within the bound.
A program may use at most 128 MiB of HBM per device.

```python
import math
import jax
import jax.numpy as jnp
import numpy as np
from jax import lax

D = 2048
FF = 1024
W = 1024
LRU_BLOCK = 64
TOK_DEV = 192
EXPERTS = 8
CAP = 96
TOKENS = 1536
FF_PART = 256
BLOCKS = 16
N_SP = 8
N_TP = 4


def draw_conv_out(key, part):
    noise_key, offset_key = jax.random.split(key, 2)
    offsets = jax.random.uniform(offset_key, (TOKENS // 64,), jnp.float32, -1.5, 1.5)
    shifts = jnp.repeat(offsets, 64)[:, None]
    base_values = jax.random.normal(noise_key, (TOKENS, W), jnp.float32)
    return jnp.clip(base_values + shifts, -6.0, 6.0).astype(jnp.bfloat16)


def draw_decay_param(key, part):
    pick_key, slow_key, fast_key = jax.random.split(key, 3)
    chooser = jax.random.uniform(pick_key, (W,), jnp.float32)
    slow_values = jnp.log(TOKENS * 1.0) + jax.random.uniform(slow_key, (W,), jnp.float32, 1.5, 3.0)
    fast_values = jax.random.uniform(fast_key, (W,), jnp.float32, 4.8, 6.0)
    slow_share = 0.5
    return jnp.where(chooser < slow_share, slow_values, fast_values).astype(jnp.float32)


def spiked(drawn, own_key, source, target, shards_of, factor):
    def block_of(position):
        return (jnp.arange(drawn.shape[position]) // (drawn.shape[position] // shards_of)).reshape((-1,) + (1,) * (drawn.ndim - 1 - position))

    near = jax.random.permutation(own_key, shards_of)[block_of(target)]
    second = (block_of(target) + shards_of // 2) % shards_of
    return jnp.where((block_of(source) == near) | (block_of(source) == second), factor * drawn, drawn)


def block_scale(own_key, dims, cuts, smallest, high):
    level = 1.0
    for axis_at, shards_of in cuts:
        heights = jax.random.uniform(jax.random.fold_in(jax.random.fold_in(own_key, 6), axis_at), (shards_of,), jnp.float32, smallest / len(cuts), high / len(cuts))
        level = level * jnp.repeat(jnp.exp(heights), dims[axis_at] // shards_of).reshape((-1,) + (1,) * (len(dims) - 1 - axis_at))
    return level


def assign_block(own_key, own, number, rows, number_of, top, limit, skew):
    order = jax.random.permutation(own_key, number_of)
    crowded, common = portions_of(number_of, rows * top, limit, skew, True), portions_of(number_of, rows * top, limit, skew, False)
    places = jnp.arange(number_of)

    def named(sizes, rotation):
        used = int((sizes > 0).sum())
        fixed = max(1, used // 4)
        moved = fixed + (places - fixed + rotation * (used - fixed)) % max(1, number_of - fixed)
        return jnp.zeros((number_of,), jnp.int32).at[order[jnp.where(places < fixed, places, moved)]].set(jnp.asarray(sizes, jnp.int32))

    sizes = jnp.where(number % 4 == 0, named(crowded, number // 4), named(common, number - number // 4 - 1))
    mixed = jax.random.permutation(jax.random.fold_in(own, 3), number_of)
    giver, receiver = mixed[0:number_of // 2 * 2:2], mixed[1:number_of // 2 * 2:2]
    margin = jnp.minimum(sizes[giver] - 1, limit - sizes[receiver]) // 2
    margin = jnp.where((giver == order[0]) | (receiver == order[0]) | (sizes[receiver] == 0), 0, jnp.maximum(margin, 0))
    moved = jax.random.randint(jax.random.fold_in(own, 4), (number_of // 2,), 0, 1 << 20) % (margin + 1)
    sizes = sizes.at[giver].add(-moved).at[receiver].add(moved)
    labels = jnp.searchsorted(jnp.cumsum(sizes), jnp.arange(rows * top), side="right").astype(jnp.int32)
    listing = labels.reshape(top, rows).T
    listing = listing[jax.random.permutation(jax.random.fold_in(own, 1), rows)]
    rotation = jax.random.randint(jax.random.fold_in(own, 2), (rows, 1), 0, top)
    return jnp.take_along_axis(listing, (jnp.arange(top)[None, :] + rotation) % top, axis=1)


def portions_of(amount, total, limit, skew, full):
    portions = [(1 << 20) // math.isqrt(rank ** skew) + 1 for rank in range(1, amount + 1)]
    largest = limit if full else min(limit, max(-(-total // amount), total * portions[0] // sum(portions)))
    least = 1 if total - largest >= amount - 1 else 0
    holding, surplus = [largest] + [least] * (amount - 1), total - largest - least * (amount - 1)
    while surplus > 0:
        movable = [i for i in range(1, amount) if holding[i] < largest] or [i for i in range(1, amount) if holding[i] < limit]
        pool, left = sum([portions[i] for i in movable]), surplus
        for i in movable:
            extra = min(limit - holding[i], max(1, left * portions[i] // pool), surplus)
            holding[i] = holding[i] + extra
            surplus = surplus - extra
    return np.array(holding)


def centred(key, extent, scale, bound, shards=(), kind=jnp.bfloat16):
    loudness = block_scale(key, extent, shards, -0.22, 0.18) if shards else 1.0
    array = jax.random.normal(key, extent, jnp.float32) * scale * loudness
    return jnp.minimum(jnp.maximum(array, -bound), bound).astype(kind)


def gaussian_with(stream_key, extent, scale, limit, cuts, heavy, held_as=jnp.bfloat16):
    drawn = scale * jax.random.normal(stream_key, extent, jnp.float32)
    if cuts:
        drawn = drawn * block_scale(stream_key, extent, cuts, -0.22, 0.18)
    return jnp.clip(spiked(drawn, jax.random.fold_in(stream_key, 3), *heavy), -limit, limit).astype(held_as)


def setup_inputs(seed: int = 0) -> dict:
    streams_of = jax.random.split(jax.random.key(seed), 16)
    cotangent = gaussian_with(streams_of[0], (TOKENS, D), 1.0, 8.0, ((0, 8),), (0, 1, 8, 2.0))
    residual = centred(streams_of[1], (TOKENS, D), 1.0, 6.0, ((0, 8),))
    norm_gain = jnp.clip(1.0 + 0.18 * jax.random.normal(streams_of[2], (D,), jnp.float32), 0.1, 1.9)
    route_ids_keys = jax.random.split(jax.random.fold_in(streams_of[3], 1), TOKENS // TOK_DEV)
    route_ids_turns = jax.random.permutation(jax.random.fold_in(streams_of[3], 3), TOKENS // TOK_DEV)
    route_ids = jax.vmap(lambda own, number: assign_block(jax.random.fold_in(streams_of[3], 2), own, number, TOK_DEV, EXPERTS, 2, CAP, 1))(route_ids_keys, route_ids_turns).reshape((TOKENS, 2))
    route_weights = jnp.clip(0.1 + 0.9 * jax.random.uniform(streams_of[4], (TOKENS, 2), jnp.float32) ** block_scale(streams_of[4], (TOKENS, 2), ((0, 8),), -0.2, 0.2), 0.1, 1.0)
    expert_gate = centred(streams_of[5], (EXPERTS, D, FF), D ** -0.5, 0.125, ((0, 8), (2, 4)))
    expert_up = centred(streams_of[6], (EXPERTS, D, FF), D ** -0.5, 0.125, ((0, 8), (2, 4)))
    expert_down = centred(streams_of[7], (EXPERTS, FF, D), FF ** -0.5, 0.1875, ((0, 8), (1, 4)))
    out_proj = centred(streams_of[8], (D, W), W ** -0.5, 0.1875, ((1, 4),))
    conv_out = draw_conv_out(jax.random.fold_in(streams_of[15], 71), 0)
    branch_gate = centred(streams_of[10], (TOKENS, W), 1.0, 6.0, ((0, 8), (1, 4)))
    prev_state = centred(streams_of[11], (TOKENS, W), 1.0, 6.0, ((0, 8), (1, 4)))
    decay_param = draw_decay_param(jax.random.fold_in(streams_of[15], 71), 0)
    rate_map = centred(streams_of[13], (BLOCKS, LRU_BLOCK, LRU_BLOCK), LRU_BLOCK ** -0.5, 0.75, ((0, 4),))
    input_map = centred(streams_of[14], (BLOCKS, LRU_BLOCK, LRU_BLOCK), LRU_BLOCK ** -0.5, 0.75, ((0, 4),))
    return {"cotangent": cotangent, "residual": residual, "norm_gain": norm_gain, "route_ids": route_ids, "route_weights": route_weights, "expert_gate": expert_gate, "expert_up": expert_up, "expert_down": expert_down, "out_proj": out_proj, "conv_out": conv_out, "branch_gate": branch_gate, "prev_state": prev_state, "decay_param": decay_param, "rate_map": rate_map, "input_map": input_map}


RATE_SCALE = 8.0
NORM_EPS = 1e-06
SERIES_EDGE = 0.001

def gelu_pair(values):
    result, pullback = jax.vjp(jax.nn.gelu, values)
    return (result, pullback(jnp.ones_like(values))[0])

def gate_maps(conv_out, weights):
    rows_here = conv_out.shape[0]
    blocked = conv_out.astype(jnp.float32).reshape(rows_here, weights.shape[0], weights.shape[1])
    mapped = jnp.einsum('tbi,bij->tbj', blocked, weights.astype(jnp.float32))
    return mapped.reshape(rows_here, -1)

def gate_maps_back(grad_values, weights):
    rows_here = grad_values.shape[0]
    blocked = grad_values.reshape(rows_here, weights.shape[0], weights.shape[2])
    mapped = jnp.einsum('tbj,bij->tbi', blocked, weights.astype(jnp.float32), precision=lax.Precision.HIGHEST)
    return mapped.reshape(rows_here, -1)

def norm_slope(spread):
    tiny_side = spread < SERIES_EDGE
    denominator = jnp.where(tiny_side, 1.0, -jnp.expm1(-spread))
    series_ratio = jnp.where(tiny_side, 1.0 + 0.5 * spread, spread / denominator)
    return 0.5 * jnp.sqrt(spread * series_ratio)

def reverse_linear(factors, term_values):

    def combine(left_pair, right_pair):
        return (left_pair[0] * right_pair[0], right_pair[0] * left_pair[1] + right_pair[1])
    flipped = lax.associative_scan(combine, (jnp.flip(factors, 0), jnp.flip(term_values, 0)), axis=0)
    return jnp.flip(flipped[1], 0)

def reference(cotangent, residual, norm_gain, route_ids, route_weights, expert_gate, expert_up, expert_down, out_proj, conv_out, branch_gate, prev_state, decay_param, rate_map, input_map):
    res_values = residual.astype(jnp.float32)
    inv_rms = lax.rsqrt(lax.optimization_barrier(jnp.mean(res_values * res_values, axis=1, keepdims=True)) + NORM_EPS)
    moe_input = (res_values * inv_rms * norm_gain[None, :]).astype(jnp.bfloat16)
    scaled_cot = (route_weights[:, :, None] * cotangent.astype(jnp.float32)[:, None, :]).astype(jnp.bfloat16)
    scaled_cot = scaled_cot.reshape(2 * TOKENS, D)
    id_blocks = route_ids.reshape(N_SP, 2 * TOK_DEV)
    expert_hits = (id_blocks[:, :, None] == jnp.arange(EXPERTS, dtype=jnp.int32)[None, None, :]).astype(jnp.int32)
    earlier_hits = jnp.cumsum(expert_hits, axis=1) - expert_hits
    rank_in = lax.optimization_barrier(jnp.sum(earlier_hits * expert_hits, axis=2))
    global_slot = (id_blocks * (N_SP * CAP) + jnp.arange(N_SP, dtype=jnp.int32)[:, None] * CAP + rank_in).reshape(-1).astype(jnp.int32)
    slot_total = EXPERTS * N_SP * CAP
    assign_table = jnp.zeros((slot_total,), jnp.int32).at[global_slot].set(jnp.arange(2 * TOKENS, dtype=jnp.int32)).reshape(EXPERTS, N_SP * CAP)
    filled_table = jnp.zeros((slot_total,), jnp.int32).at[global_slot].set(1).reshape(EXPERTS, N_SP * CAP)

    def one_expert(packed):
        gate_one, up_one, down_one, assign_one, filled_one = packed
        rows_in = moe_input[assign_one // 2]
        cot_in = jnp.where(filled_one[:, None] > 0, scaled_cot[assign_one], jnp.zeros((), jnp.bfloat16))
        gate_pre = jnp.dot(rows_in, gate_one, preferred_element_type=jnp.float32)
        up_pre = jnp.dot(rows_in, up_one, preferred_element_type=jnp.float32)
        gate_sig = jax.nn.sigmoid(gate_pre)
        gate_act = gate_pre * gate_sig
        hidden = (gate_act * up_pre).astype(jnp.bfloat16)
        d_hidden = jnp.dot(cot_in, down_one.T, preferred_element_type=jnp.float32)
        d_up = (d_hidden * gate_act).astype(jnp.bfloat16)
        d_gate = (d_hidden * up_pre * gate_sig * (1.0 + gate_pre * (1.0 - gate_sig))).astype(jnp.bfloat16)
        grad_down_one = jnp.dot(hidden.T, cot_in, preferred_element_type=jnp.float32)
        grad_gate_one = jnp.dot(rows_in.T, d_gate, preferred_element_type=jnp.float32)
        grad_up_one = jnp.dot(rows_in.T, d_up, preferred_element_type=jnp.float32)
        rows_count = rows_in.shape[0]
        gate_blocks = d_gate.astype(jnp.float32).reshape(rows_count, N_TP, FF_PART)
        up_blocks = d_up.astype(jnp.float32).reshape(rows_count, N_TP, FF_PART)
        block_terms = jnp.einsum('rnf,dnf->nrd', gate_blocks, gate_one.astype(jnp.float32).reshape(D, N_TP, FF_PART))
        block_terms = block_terms + jnp.einsum('rnf,dnf->nrd', up_blocks, up_one.astype(jnp.float32).reshape(D, N_TP, FF_PART))
        rounded = lax.optimization_barrier(block_terms.astype(jnp.bfloat16))
        expert_back_one = lax.optimization_barrier(jnp.sum(rounded.astype(jnp.float32), axis=0)).astype(jnp.bfloat16)
        return (grad_gate_one, grad_up_one, grad_down_one, expert_back_one)
    grad_gate, grad_up, grad_down, expert_back = lax.map(one_expert, (expert_gate, expert_up, expert_down, assign_table, filled_table))
    back_rows = expert_back.reshape(slot_total, D)[global_slot].astype(jnp.float32)
    d_normed = lax.optimization_barrier(jnp.sum(back_rows.reshape(TOKENS, 2, D), axis=1))
    weighted = norm_gain[None, :] * d_normed
    cubed = inv_rms * inv_rms * inv_rms
    d_mix = (cotangent.astype(jnp.float32) + inv_rms * weighted - res_values * cubed * lax.optimization_barrier(jnp.mean(res_values * weighted, axis=1, keepdims=True))).astype(jnp.bfloat16)
    rate_gate = jax.nn.sigmoid(gate_maps(conv_out, rate_map))
    input_gate = jax.nn.sigmoid(gate_maps(conv_out, input_map))
    soft_decay = jax.nn.softplus(-decay_param)
    log_keep = -RATE_SCALE * rate_gate * soft_decay[None, :]
    keep_rate = jnp.exp(log_keep)
    spread = -2.0 * log_keep
    norm_term = jnp.sqrt(-jnp.expm1(-spread))
    conv_values = conv_out.astype(jnp.float32)
    prev_values = prev_state.astype(jnp.float32)
    state_now = keep_rate * prev_values + norm_term * input_gate * conv_values
    gelu_value, gelu_slope = gelu_pair(branch_gate.astype(jnp.float32))
    branch_out = (state_now * gelu_value).astype(jnp.bfloat16)
    grad_out_proj = lax.dot_general(d_mix, branch_out, (((0,), (0,)), ((), ())), preferred_element_type=jnp.float32)
    d_branch = jnp.dot(d_mix, out_proj, preferred_element_type=jnp.float32)
    next_keep = jnp.concatenate([keep_rate[1:], jnp.zeros_like(keep_rate[:1])], axis=0)
    state_grad = reverse_linear(next_keep, d_branch * gelu_value)
    grad_branch_gate = d_branch * state_now * gelu_slope
    keep_grad = state_grad * prev_values * keep_rate
    inner_input = input_gate * conv_values
    rate_back = keep_grad * (-RATE_SCALE * soft_decay[None, :]) * rate_gate * (1.0 - rate_gate)
    rate_back = rate_back + state_grad * inner_input * keep_rate * keep_rate * (1.0 - rate_gate) * norm_slope(spread)
    input_back = state_grad * norm_term * conv_values * input_gate * (1.0 - input_gate)
    grad_conv_out = state_grad * norm_term * input_gate + gate_maps_back(rate_back, rate_map) + gate_maps_back(input_back, input_map)
    return (grad_gate, grad_up, grad_down, grad_out_proj, grad_conv_out, grad_branch_gate)
```

```python
import contextlib

import jax
import jax.numpy as jnp
from jax import lax
from jax.sharding import PartitionSpec as P
from jax.experimental import pallas as pl
from jax.experimental.pallas import tpu as pltpu

RATE_SCALE = 8.0
NORM_EPS = 1e-06
SERIES_EDGE = 0.001
MESH = pl.DeviceIdType.MESH
SCOPES = False
OVER_ROWS = (((0,), (0,)), ((), ()))
OVER_COLS = (((1,), (1,)), ((), ()))


def scope(name):
    return jax.named_scope(name) if SCOPES else contextlib.nullcontext()


def partner_of(place, i, count):
    total = lax.rem(place + i, 2)
    bit = 2
    while bit < count:
        own = lax.div(place, bit) + lax.div(i, bit) + lax.div(i, 2 * bit)
        total = total + bit * lax.rem(own, 2)
        bit *= 2
    return total


def remote(src, dst, send_sem, recv_sem, device):
    return pltpu.make_async_remote_copy(
        src_ref=src,
        dst_ref=dst,
        send_sem=send_sem,
        recv_sem=recv_sem,
        device_id=device,
        device_id_type=MESH,
    )


def one_less_exp(spread):
    small = jnp.minimum(spread, 0.3)
    series = jnp.full_like(small, 1.0 / 40320.0)
    for factorial in (5040.0, 720.0, 120.0, 24.0, 6.0, 2.0, 1.0):
        series = 1.0 / factorial - small * series
    return jnp.where(spread < 0.3, small * series, 1.0 - jnp.exp(-spread))


def loop(begin, end, step):
    def body(i, carry):
        step(i)
        return carry

    lax.fori_loop(begin, end, body, 0)


def layer_kernel(
    sp_count,
    tp_count,
    refs_in,
    gate_grad,
    up_grad,
    down_grad,
    proj_grad,
    conv_grad,
    branch_grad,
    refs_here,
    maps,
    sending,
    moe_part,
    scaled_first,
    scaled_second,
    pre_values,
    held,
    part,
    from_beside,
    to_across,
    from_across,
    mine,
    leaving,
    arrived,
    full,
    hidden,
    d_gate,
    d_up,
    rate_factor,
    input_factor,
    direct_factor,
    gate_factor,
    gelu_values,
    keep,
    branch_all,
    mix,
    share,
    mix_all,
    small,
    small_all,
    load_sem,
    send_sem,
    recv_sem,
    back_send,
    back_recv,
    branch_send,
    branch_recv,
    last_send,
    last_recv,
    share_send,
    share_recv,
    small_send,
    small_recv,
):
    s = lax.axis_index("sp")
    t = lax.axis_index("tp")
    beside = t + 1 - 2 * lax.rem(t, 2)
    across = lax.rem(t + tp_count // 2, tp_count)
    facing = lax.rem(beside + tp_count // 2, tp_count)
    half = sp_count // 2
    s_twin = s + 1 - 2 * lax.rem(s, 2)
    (res, cot, gain, ids, weights, conv, gate, prev, decay, rate_map, input_map) = refs_here[:11]
    gate_w, up_w, down_w, proj = refs_here[11:]
    tok_rows, model_width = res.shape
    cap, width = sending.shape[2:]
    channels = conv.shape[1]
    share_rows, out_rows = share.shape[1:]

    def partner(i):
        return partner_of(s, i, sp_count)

    barrier = pltpu.get_barrier_semaphore()
    for other in (beside, across):
        pl.semaphore_signal(barrier, inc=1, device_id=(s, other), device_id_type=MESH)
    loop(
        1,
        sp_count,
        lambda i: pl.semaphore_signal(
            barrier, inc=1, device_id=(partner(i), t), device_id_type=MESH
        ),
    )
    loads = [
        pltpu.make_async_copy(src, dst, load_sem.at[k])
        for k, (src, dst) in enumerate(zip(refs_in, refs_here))
    ]
    for copy in loads:
        copy.start()
    for copy in loads[:5]:
        copy.wait()

    def cols_of(q):
        return pl.ds(pl.multiple_of(q * width, width), width)

    with scope("prepare"):
        cols = cols_of(t)
        res_all = res[...].astype(jnp.float32)
        inv_rms = lax.rsqrt(jnp.mean(res_all * res_all, axis=1, keepdims=True) + NORM_EPS)
        moe_part[...] = (res[:, cols].astype(jnp.float32) * inv_rms * gain[:, cols]).astype(
            jnp.bfloat16
        )
        square = (tok_rows, tok_rows)
        down_at = lax.broadcasted_iota(jnp.int32, square, 0)
        over_at = lax.broadcasted_iota(jnp.int32, square, 1)

        def column(row):
            return jnp.sum(jnp.where(down_at == over_at, row, 0.0), axis=1, keepdims=True)

        cot_mine = cot[:, cols].astype(jnp.float32)
        scaled_first[...] = (column(weights[0:1, :]) * cot_mine).astype(jnp.bfloat16)
        scaled_second[...] = (column(weights[1:2, :]) * cot_mine).astype(jnp.bfloat16)
        experts = lax.broadcasted_iota(jnp.int32, (sp_count, tok_rows), 0)
        is_first = ids[0:1, :] == experts
        is_second = ids[1:2, :] == experts
        hits = (is_first | is_second).astype(jnp.float32).astype(jnp.bfloat16)
        earlier = (down_at < over_at).astype(jnp.float32).astype(jnp.bfloat16)
        ranks = jnp.dot(hits, earlier, preferred_element_type=jnp.float32)
        row_first = jnp.sum(jnp.where(is_first, ranks, 0.0), axis=0, keepdims=True)
        row_second = jnp.sum(jnp.where(is_second, ranks, 0.0), axis=0, keepdims=True)
        row_first = row_first + (ids[0:1, :] * cap).astype(jnp.float32)
        row_second = row_second + (ids[1:2, :] * cap).astype(jnp.float32)
        slots = lax.broadcasted_iota(jnp.int32, (cap, tok_rows), 0).astype(jnp.float32)

    def filled(target):
        base = (target * cap).astype(jnp.float32)
        first = jnp.where(row_first - base == slots, 1.0, 0.0)
        second = jnp.where(row_second - base == slots, 1.0, 0.0)
        rows = jnp.dot(
            (first + second).astype(jnp.bfloat16),
            moe_part[...],
            preferred_element_type=jnp.float32,
        ).astype(jnp.bfloat16)
        from_first = jnp.dot(
            first.astype(jnp.bfloat16), scaled_first[...], preferred_element_type=jnp.float32
        )
        from_second = jnp.dot(
            second.astype(jnp.bfloat16), scaled_second[...], preferred_element_type=jnp.float32
        )
        return rows, (from_first + from_second).astype(jnp.bfloat16)

    def quarter_of(source, q):
        return held.at[source, :, :, cols_of(q)]

    def first(i):
        target = partner(i)
        return remote(
            sending.at[target], quarter_of(s, t), send_sem.at[0], recv_sem.at[0, i], (target, t)
        )

    def passed(kind, i, q, to):
        block = quarter_of(partner(i), q)
        landing = recv_sem.at[min(kind, 2), i]
        return remote(block, block, send_sem.at[kind], landing, (s, to))

    def landed(i):
        source = partner(i)
        remote(
            sending.at[source],
            quarter_of(source, t),
            send_sem.at[0],
            recv_sem.at[0, i],
            (source, t),
        ).wait_recv()

    def pass_on(i):
        passed(1, i, t, across).start()
        passed(2, i, t, beside).start()

    def pass_back(i):
        passed(1, i, across, across).wait_recv()
        passed(3, i, across, beside).start()

    def all_of(like, sem):
        return remote(like, like, sem, sem, (s, beside))

    def complete(i):
        all_of(sending.at[pl.ds(0, 2)], recv_sem.at[2, i]).wait_recv()

    rows_own, cot_own = filled(s)
    held[s, 0, :, cols] = rows_own
    held[s, 1, :, cols] = cot_own
    with scope("barrier"):
        pl.semaphore_wait(barrier, sp_count + 1)
    pass_on(0)

    def send_one(i):
        target = partner(i)
        rows, values = filled(target)
        sending[target, 0] = rows
        sending[target, 1] = values
        first(i).start()

    early = min(5, sp_count)
    with scope("sends"):
        loop(1, early, send_one)

    for copy in loads[5:11]:
        copy.wait()
    with scope("forward"):
        block = rate_map.shape[1]
        lane_in = lax.rem(lax.broadcasted_iota(jnp.int32, (block, channels), 1), block)
        spread_out = lane_in == lax.broadcasted_iota(jnp.int32, (block, channels), 0)
        spread_out = spread_out.astype(jnp.float32).astype(jnp.bfloat16)
        wide = (channels, channels)
        same = lax.div(lax.broadcasted_iota(jnp.int32, wide, 0), block) == lax.div(
            lax.broadcasted_iota(jnp.int32, wide, 1), block
        )
        for k, blocks in enumerate((rate_map, input_map)):
            tiled = jnp.dot(
                blocks[...].reshape(channels, block),
                spread_out,
                preferred_element_type=jnp.float32,
            )
            maps[:, k * channels : (k + 1) * channels] = jnp.where(same, tiled, 0.0).astype(
                jnp.bfloat16
            )
        pre_values[...] = jnp.dot(conv[...], maps[...], preferred_element_type=jnp.float32)
        y = jnp.exp(-decay[...])
        soft = y * (1.0 - y * (0.5 - y * (1.0 / 3.0 - y * (0.25 - y * 0.2))))
        step = 16

        def forward(i):
            rows = pl.ds(pl.multiple_of(i * step, step), step)
            rate_gate = jax.nn.sigmoid(pre_values[rows, :channels])
            input_gate = jax.nn.sigmoid(pre_values[rows, channels:])
            log_keep = -RATE_SCALE * rate_gate * soft
            kept = jnp.exp(log_keep)
            spread = -2.0 * log_keep
            gone = one_less_exp(spread)
            norm_term = jnp.sqrt(gone)
            conv_values = conv[rows, :].astype(jnp.float32)
            prev_values = prev[rows, :].astype(jnp.float32)
            inner = input_gate * conv_values
            state_now = kept * prev_values + norm_term * inner
            v = gate[rows, :].astype(jnp.float32)
            root = 0.7978845608028654
            bent = jnp.tanh(root * (v + 0.044715 * v * v * v))
            gelu_value = 0.5 * v * (1.0 + bent)
            gelu_slope = 0.5 * (1.0 + bent) + 0.5 * v * (1.0 - bent * bent) * root * (
                1.0 + 3.0 * 0.044715 * v * v
            )
            tiny_side = spread < SERIES_EDGE
            series = jnp.where(
                tiny_side, 1.0 + 0.5 * spread, spread / jnp.where(tiny_side, 1.0, gone)
            )
            slope = 0.5 * jnp.sqrt(spread * series)
            branch_all[s, rows, :] = (state_now * gelu_value).astype(jnp.bfloat16)
            rate_factor[rows, :] = prev_values * kept * (-RATE_SCALE * soft) * rate_gate * (
                1.0 - rate_gate
            ) + inner * kept * kept * (1.0 - rate_gate) * slope
            input_factor[rows, :] = norm_term * conv_values * input_gate * (1.0 - input_gate)
            direct_factor[rows, :] = norm_term * input_gate
            gate_factor[rows, :] = state_now * gelu_slope
            gelu_values[rows, :] = gelu_value
            keep[rows, :] = kept

        loop(0, tok_rows // step, forward)

    for copy in loads[11:]:
        copy.wait()

    def to_beside(i, k):
        source = partner(i)
        q = beside if k == 0 else facing
        return remote(
            part.at[source, :, cols_of(q)],
            from_beside.at[k, source],
            back_send.at[k],
            back_recv.at[k, i],
            (s, beside),
        )

    def crossing(i):
        source = partner(i)
        return remote(
            to_across.at[source],
            from_across.at[source],
            back_send.at[2],
            back_recv.at[2, i],
            (s, across),
        )

    def homeward(i):
        source = partner(i)
        return remote(
            leaving.at[source],
            arrived.at[s],
            back_send.at[3],
            back_recv.at[3, i],
            (source, t),
        )

    def expert(i):
        complete(i)
        source = partner(i)
        rows_in = held[source, 0]
        gate_pre = jnp.dot(rows_in, gate_w[...], preferred_element_type=jnp.float32)
        up_pre = jnp.dot(rows_in, up_w[...], preferred_element_type=jnp.float32)
        d_hidden = lax.dot_general(
            held[source, 1], down_w[...], OVER_COLS, preferred_element_type=jnp.float32
        )
        gate_sig = jax.nn.sigmoid(gate_pre)
        gate_act = gate_pre * gate_sig
        up_back = (d_hidden * gate_act).astype(jnp.bfloat16)
        gate_back = (d_hidden * up_pre * gate_sig * (1.0 + gate_pre * (1.0 - gate_sig))).astype(
            jnp.bfloat16
        )
        hidden[source] = (gate_act * up_pre).astype(jnp.bfloat16)
        d_up[source] = up_back
        d_gate[source] = gate_back
        back = lax.dot_general(
            gate_back, gate_w[...], OVER_COLS, preferred_element_type=jnp.float32
        )
        back = back + lax.dot_general(
            up_back, up_w[...], OVER_COLS, preferred_element_type=jnp.float32
        )
        part[source] = back.astype(jnp.bfloat16)
        to_beside(i, 1).start()
        to_beside(i, 0).start()

    def cross(i):
        to_beside(i, 1).wait_recv()
        at = partner(i)
        total = part[at, :, cols_of(across)].astype(jnp.float32) + from_beside[1, at].astype(
            jnp.float32
        )
        to_across[at] = total.astype(jnp.bfloat16)
        crossing(i).start()
        to_beside(i, 0).wait_recv()
        mine[at] = part[at, :, cols].astype(jnp.float32) + from_beside[0, at].astype(jnp.float32)

    def leave(i):
        crossing(i).wait_recv()
        at = partner(i)
        total = (mine[at] + from_across[at].astype(jnp.float32)).astype(jnp.bfloat16)

        @pl.when(i > 0)
        def _():
            leaving[at] = total
            homeward(i).start()

        @pl.when(i == 0)
        def _():
            arrived[s] = total

    def turn(i):
        @pl.when((i >= 2) & (i < sp_count + 2))
        def _():
            with scope("expert"):
                expert(i - 2)

        @pl.when(i >= 4)
        def _():
            with scope("leave"):
                leave(i - 4)

        @pl.when((i >= 1) & (i < sp_count))
        def _():
            with scope("landed"):
                landed(i)
            pass_on(i)

        @pl.when((i >= 1) & (i + early - 1 < sp_count))
        def _():
            send_one(i + early - 1)

        @pl.when((i >= 1) & (i < sp_count + 1))
        def _():
            with scope("pass_back"):
                pass_back(i - 1)

        @pl.when((i >= 2) & (i < sp_count + 2))
        def _():
            with scope("cross"):
                cross(i - 2)

    loop(0, sp_count + 4, turn)

    own_branch = branch_all.at[s]

    def branch_copy(j):
        return remote(
            own_branch,
            own_branch,
            branch_send.at[0],
            branch_recv.at[j],
            (partner(2 * j), t),
        )

    def branch_landed(j):
        source = partner(2 * j)
        return remote(
            own_branch,
            branch_all.at[source],
            branch_send.at[0],
            branch_recv.at[j],
            (source, t),
        )

    def branch_twin(j):
        block = branch_all.at[partner(2 * j)]
        return remote(block, block, branch_send.at[1], branch_recv.at[0], (s_twin, t))

    def merged(values):
        return values.reshape(sp_count * cap, values.shape[2])

    def summed(left, right):
        if cap % 16 == 0:
            return lax.dot_general(
                merged(left), merged(right), OVER_ROWS, preferred_element_type=jnp.float32
            )
        total = None
        for source in range(sp_count):
            one = lax.dot_general(
                left[source], right[source], OVER_ROWS, preferred_element_type=jnp.float32
            )
            total = one if total is None else total + one
        return total

    tile = 256
    def rows_tile(k):
        at = pl.ds(pl.multiple_of(k * tile, tile), tile)
        rows = held[:, 0, :, at]
        gate_grad[at, :] = summed(rows, d_gate[...])
        up_grad[at, :] = summed(rows, d_up[...])

    def cot_tile(k):
        at = pl.ds(pl.multiple_of(k * tile, tile), tile)
        down_grad[:, at] = summed(hidden[...], held[:, 1, :, at])

    with scope("grads_rows"):
        loop(0, model_width // tile, rows_tile)

    lanes = lax.broadcasted_iota(jnp.int32, (tok_rows, cap), 1).astype(jnp.float32)
    slot_first, slot_second = column(row_first), column(row_second)

    def gather_rows(source):
        base = (source * cap).astype(jnp.float32)
        chosen = jnp.where(slot_first - base == lanes, 1.0, 0.0)
        chosen = chosen + jnp.where(slot_second - base == lanes, 1.0, 0.0)
        return jnp.dot(
            chosen.astype(jnp.bfloat16), arrived[source], preferred_element_type=jnp.float32
        )

    def add_in(i, total):
        source = partner(i)
        with scope("home"):
            remote(
                leaving.at[source],
                arrived.at[source],
                back_send.at[3],
                back_recv.at[3, i],
                (source, t),
            ).wait_recv()
        return total + gather_rows(source)

    full[:, cols] = lax.fori_loop(1, sp_count, add_in, gather_rows(s)).astype(jnp.bfloat16)

    def gathered(kind, q, to):
        block = full.at[:, cols_of(q)]
        return remote(block, block, last_send.at[kind], last_recv.at[kind], (s, to))

    gathered(0, t, across).start()
    gathered(1, t, beside).start()
    loop(1, half, lambda j: branch_copy(j).start())
    branch_twin(0).start()
    with scope("grads_cot"):
        loop(0, model_width // tile, cot_tile)
    with scope("quarter"):
        gathered(0, across, across).wait_recv()
        gathered(2, across, beside).start()
        gathered(1, beside, beside).wait_recv()
        gathered(2, facing, beside).wait_recv()

    def mix_rows(begin):
        rows = pl.ds(pl.multiple_of(begin, share_rows), share_rows)
        values = res[rows, :].astype(jnp.float32)
        weighted = gain[...] * full[rows, :].astype(jnp.float32)
        inverse = lax.rsqrt(jnp.mean(values * values, axis=1, keepdims=True) + NORM_EPS)
        cubed = inverse * inverse * inverse
        slope = cubed * jnp.mean(values * weighted, axis=1, keepdims=True)
        return rows, (
            cot[rows, :].astype(jnp.float32) + inverse * weighted - values * slope
        ).astype(jnp.bfloat16)

    def share_view(source, q):
        return mix_all.at[source, pl.ds(pl.multiple_of(q * share_rows, share_rows), share_rows), :]

    def share_first(i):
        target = partner(i)
        return remote(
            share.at[target],
            share_view(s, t),
            share_send.at[0],
            share_recv.at[0, i],
            (target, t),
        )

    def share_passed(kind, i, q, to):
        block = share_view(partner(i), q)
        landing = share_recv.at[1, i] if kind == 1 else share_recv.at[0, 0]
        return remote(block, block, share_send.at[kind], landing, (s, to))

    def share_landed(i):
        source = partner(i)
        remote(
            share.at[source],
            share_view(source, t),
            share_send.at[0],
            share_recv.at[0, i],
            (source, t),
        ).wait_recv()

    def share_on(i):
        share_passed(1, i, t, across).start()
        share_passed(2, i, t, beside).start()

    def share_back(i):
        share_passed(1, i, across, across).wait_recv()
        share_passed(3, i, across, beside).start()

    with scope("share"):
        _, own_rows = mix_rows(t * share_rows)
        for j in range(sp_count):
            share[j] = own_rows[:, j * out_rows : (j + 1) * out_rows]
        loop(1, sp_count, lambda i: share_first(i).start())
        own_at = pl.ds(pl.multiple_of(t * share_rows, share_rows), share_rows)
        mix_all[s, own_at, :] = share[s]
        share_on(0)

    with scope("branch_pass"):

        def pass_branch(j):
            branch_landed(j).wait_recv()
            branch_twin(j).start()

        loop(1, half, pass_branch)
    with scope("mix"):

        def fill(k):
            rows, values = mix_rows(k * share_rows)
            mix[rows, :] = values

        loop(0, tp_count, fill)

    with scope("scan"):
        d_branch = jnp.dot(mix[...], proj[...], preferred_element_type=jnp.float32)
        branch_grad[...] = d_branch * gate_factor[...]
        at = lax.broadcasted_iota(jnp.int32, d_branch.shape, 0)
        grads = d_branch * gelu_values[...]
        keeps = jnp.where(at < tok_rows - 1, pltpu.roll(keep[...], tok_rows - 1, 0), 1.0)
        reach = 1
        while reach < tok_rows:
            inside = at < tok_rows - reach
            later_grads = jnp.where(inside, pltpu.roll(grads, tok_rows - reach, 0), 0.0)
            later_keeps = jnp.where(inside, pltpu.roll(keeps, tok_rows - reach, 0), 1.0)
            grads = grads + keeps * later_grads
            keeps = keeps * later_keeps
            reach *= 2
        small[...] = jnp.zeros_like(small)
        small[0:1, :] = keep[0:1, :] * keeps[0:1, :]
        small[1:2, :] = keep[0:1, :] * grads[0:1, :]
        small_all[s] = jnp.zeros(small.shape, jnp.float32)

    def carry_to(i):
        return remote(
            small, small_all.at[s], small_send.at[0], small_recv.at[0], (partner(i), t)
        )

    loop(1, sp_count, lambda i: carry_to(i).start())

    def relay(i):
        @pl.when(i < sp_count)
        def _():
            share_landed(i)
            share_on(i)

        @pl.when(i >= 2)
        def _():
            share_back(i - 2)

    with scope("relay"):
        loop(1, sp_count + 2, relay)

    with scope("small"):
        all_of(small_all.at[pl.ds(0, sp_count - 1)], small_recv.at[0]).wait_recv()

    def compose(turn, carried):
        source = sp_count - 1 - turn
        later = small_all[source]
        return jnp.where(source > s, later[1:2] + later[0:1] * carried, carried)

    with scope("back_maps"):
        carried = lax.fori_loop(0, sp_count - 1, compose, jnp.zeros((1, channels), jnp.float32))
        state_grad = grads + keeps * carried
        back = jnp.concatenate(
            [state_grad * rate_factor[...], state_grad * input_factor[...]], axis=1
        )
        high = back.astype(jnp.bfloat16)
        low = (back - high.astype(jnp.float32)).astype(jnp.bfloat16)
        conv_grad[...] = (
            state_grad * direct_factor[...]
            + lax.dot_general(high, maps[...], OVER_COLS, preferred_element_type=jnp.float32)
            + lax.dot_general(low, maps[...], OVER_COLS, preferred_element_type=jnp.float32)
        )

    with scope("last_waits"):

        all_of(mix_all.at[:, pl.ds(0, 2 * share_rows)], share_recv.at[0, 0]).wait_recv()
        all_of(branch_all.at[pl.ds(0, half)], branch_recv.at[0]).wait_recv()
    with scope("grad_proj"):
        proj_grad[...] = lax.dot_general(
            mix_all[...].reshape(sp_count * tok_rows, out_rows),
            branch_all[...].reshape(sp_count * tok_rows, channels),
            OVER_ROWS,
            preferred_element_type=jnp.float32,
        )

    others = pl.ds(0, sp_count - 1)
    with scope("end"):
        all_of(sending.at[others], send_sem.at[0]).wait_send()
        for kind in (1, 2, 3):
            all_of(sending, send_sem.at[kind]).wait_send()
            all_of(to_across, back_send.at[kind - 1]).wait_send()
            all_of(share, share_send.at[kind]).wait_send()
        all_of(to_across.at[others], back_send.at[3]).wait_send()
        all_of(share.at[others], share_send.at[0]).wait_send()
        all_of(small_all.at[others], small_send.at[0]).wait_send()
        all_of(branch_all.at[pl.ds(0, half - 1)], branch_send.at[0]).wait_send()
        all_of(branch_all.at[pl.ds(0, half)], branch_send.at[1]).wait_send()
        gathered(0, t, across).wait_send()
        gathered(1, t, beside).wait_send()
        gathered(2, across, beside).wait_send()


def layer(sp_count, tp_count, cap, operands):
    res, conv, gate_w, down_w = (operands[k] for k in (0, 5, 11, 13))
    tok_rows, model_width = res.shape
    channels, units = conv.shape[1], down_w.shape[0]
    width = model_width // tp_count
    share_rows, out_rows = tok_rows // tp_count, model_width // sp_count
    vmem = pl.BlockSpec(memory_space=pltpu.VMEM)
    anywhere = pl.BlockSpec(memory_space=pl.ANY)
    low, exact = jnp.bfloat16, jnp.float32
    blocks = (sp_count, cap, width)
    scratch = [
        ((channels, 2 * channels), low),
        ((sp_count, 2, cap, width), low),
        ((tok_rows, width), low),
        ((tok_rows, width), low),
        ((tok_rows, width), low),
        ((tok_rows, 2 * channels), exact),
        ((sp_count, 2, cap, model_width), low),
        ((sp_count, cap, model_width), low),
        ((2,) + blocks, low),
        (blocks, low),
        (blocks, low),
        (blocks, exact),
        (blocks, low),
        (blocks, low),
        (res.shape, low),
        ((sp_count, cap, units), low),
        ((sp_count, cap, units), low),
        ((sp_count, cap, units), low),
    ]
    scratch += [(conv.shape, exact)] * 6
    scratch += [
        ((sp_count,) + conv.shape, low),
        (res.shape, low),
        ((sp_count, share_rows, out_rows), low),
        ((sp_count, tok_rows, out_rows), low),
        ((8, channels), exact),
        ((sp_count, 8, channels), exact),
    ]
    sems = [
        (len(operands),),
        (4,),
        (3, sp_count),
        (4,),
        (4, sp_count),
        (2,),
        (sp_count // 2,),
        (3,),
        (3,),
        (4,),
        (2, sp_count),
        (1,),
        (1,),
    ]
    def grouped(*refs):
        layer_kernel(sp_count, tp_count, refs[: len(operands)], *refs[len(operands) :])

    return pl.pallas_call(
        grouped,
        out_shape=[
            pltpu.VMEM(shape, exact)
            for shape in (
                gate_w.shape,
                gate_w.shape,
                down_w.shape,
                (out_rows, channels),
                conv.shape,
                conv.shape,
            )
        ],
        in_specs=[anywhere] * len(operands),
        out_specs=[vmem] * 6,
        scratch_shapes=[[pltpu.VMEM(given.shape, given.dtype) for given in operands]]
        + [pltpu.VMEM(shape, kind) for shape, kind in scratch]
        + [pltpu.SemaphoreType.DMA(shape) for shape in sems],
        compiler_params=pltpu.CompilerParams(collective_id=1, has_side_effects=True, vmem_limit_bytes=59_000_000),
        cost_estimate=pl.CostEstimate(flops=0, bytes_accessed=40_000_000, transcendentals=0),
    )(*operands)


def store_kernel(*refs):
    count = len(refs) // 2
    sems = refs[-1]
    copies = [
        pltpu.make_async_copy(refs[k], refs[count + k], sems.at[k]) for k in range(count)
    ]
    for copy in copies:
        copy.start()
    for copy in copies:
        copy.wait()


def store(values):
    return pl.pallas_call(
        store_kernel,
        out_shape=[jax.ShapeDtypeStruct(value.shape, value.dtype) for value in values],
        in_specs=[pl.BlockSpec(memory_space=pltpu.VMEM)] * len(values),
        out_specs=[pl.BlockSpec(memory_space=pl.ANY)] * len(values),
        scratch_shapes=[pltpu.SemaphoreType.DMA((len(values),))],
        compiler_params=pltpu.CompilerParams(vmem_limit_bytes=16 * 1024 * 1024),
    )(*[pltpu.with_memory_space_constraint(value, pltpu.VMEM) for value in values])


def per_device(
    cotangent,
    residual,
    norm_gain,
    route_ids,
    route_weights,
    expert_gate,
    expert_up,
    expert_down,
    out_proj,
    conv_out,
    branch_gate,
    prev_state,
    decay_param,
    rate_map,
    input_map,
):
    sp_count = lax.axis_size("sp")
    tp_count = lax.axis_size("tp")
    experts_all = expert_gate.shape[0] * sp_count
    capacity = 4 * residual.shape[0] // experts_all
    grads = layer(
        sp_count,
        tp_count,
        capacity,
        (
            residual,
            cotangent,
            norm_gain[None, :],
            route_ids.T,
            route_weights.T,
            conv_out,
            branch_gate,
            prev_state,
            decay_param[None, :],
            rate_map,
            input_map,
            expert_gate[0],
            expert_up[0],
            expert_down[0],
            out_proj,
        ),
    )
    grad_gate, grad_up, grad_down, grad_out_proj, grad_conv_out, grad_branch_gate = store(grads)
    return (
        grad_gate[None],
        grad_up[None],
        grad_down[None],
        grad_out_proj,
        grad_conv_out,
        grad_branch_gate,
    )


def solution(mesh):
    in_specs = (
        P("sp", None),
        P("sp", None),
        P(),
        P("sp", None),
        P("sp", None),
        P("sp", None, "tp"),
        P("sp", None, "tp"),
        P("sp", "tp", None),
        P(None, "tp"),
        P("sp", "tp"),
        P("sp", "tp"),
        P("sp", "tp"),
        P("tp"),
        P("tp", None, None),
        P("tp", None, None),
    )
    out_specs = (
        P("sp", None, "tp"),
        P("sp", None, "tp"),
        P("sp", "tp", None),
        P("sp", "tp"),
        P("sp", "tp"),
        P("sp", "tp"),
    )
    return jax.shard_map(
        per_device, mesh=mesh, in_specs=in_specs, out_specs=out_specs, check_vma=False
    )
```

```python
import contextlib

import jax
import jax.numpy as jnp
from jax import lax
from jax.sharding import PartitionSpec as P
from jax.experimental import pallas as pl
from jax.experimental.pallas import tpu as pltpu

RATE_SCALE = 8.0
NORM_EPS = 1e-06
SERIES_EDGE = 0.001
MESH = pl.DeviceIdType.MESH
SCOPES = False
OVER_ROWS = (((0,), (0,)), ((), ()))
OVER_COLS = (((1,), (1,)), ((), ()))


def scope(name):
    return jax.named_scope(name) if SCOPES else contextlib.nullcontext()


def partner_of(place, i, count):
    total = lax.rem(place + i, 2)
    bit = 2
    while bit < count:
        own = lax.div(place, bit) + lax.div(i, bit) + lax.div(i, 2 * bit)
        total = total + bit * lax.rem(own, 2)
        bit *= 2
    return total


def remote(src, dst, send_sem, recv_sem, device):
    return pltpu.make_async_remote_copy(
        src_ref=src,
        dst_ref=dst,
        send_sem=send_sem,
        recv_sem=recv_sem,
        device_id=device,
        device_id_type=MESH,
    )


def one_less_exp(spread):
    small = jnp.minimum(spread, 0.3)
    series = jnp.full_like(small, 1.0 / 40320.0)
    for factorial in (5040.0, 720.0, 120.0, 24.0, 6.0, 2.0, 1.0):
        series = 1.0 / factorial - small * series
    return jnp.where(spread < 0.3, small * series, 1.0 - jnp.exp(-spread))


def loop(begin, end, step):
    def body(i, carry):
        step(i)
        return carry

    lax.fori_loop(begin, end, body, 0)


def layer_kernel(
    sp_count,
    tp_count,
    refs_in,
    gate_grad,
    up_grad,
    down_grad,
    proj_grad,
    conv_grad,
    branch_grad,
    refs_here,
    maps,
    sending,
    moe_part,
    scaled_first,
    scaled_second,
    pre_values,
    held,
    part,
    from_beside,
    to_across,
    from_across,
    mine,
    leaving,
    arrived,
    full,
    hidden,
    d_gate,
    d_up,
    rate_factor,
    input_factor,
    direct_factor,
    gate_factor,
    gelu_values,
    keep,
    branch_all,
    mix,
    share,
    mix_all,
    small,
    small_all,
    load_sem,
    send_sem,
    recv_sem,
    back_send,
    back_recv,
    branch_send,
    branch_recv,
    last_send,
    last_recv,
    share_send,
    share_recv,
    small_send,
    small_recv,
):
    s = lax.axis_index("sp")
    t = lax.axis_index("tp")
    beside = t + 1 - 2 * lax.rem(t, 2)
    across = lax.rem(t + tp_count // 2, tp_count)
    facing = lax.rem(beside + tp_count // 2, tp_count)
    half = sp_count // 2
    s_twin = s + 1 - 2 * lax.rem(s, 2)
    (res, cot, gain, ids, weights, conv, gate, prev, decay, rate_map, input_map) = refs_here[:11]
    gate_w, up_w, down_w, proj = refs_here[11:]
    tok_rows, model_width = res.shape
    cap, width = sending.shape[2:]
    channels = conv.shape[1]
    share_rows, out_rows = share.shape[1:]

    def partner(i):
        return partner_of(s, i, sp_count)

    barrier = pltpu.get_barrier_semaphore()
    for other in (beside, across):
        pl.semaphore_signal(barrier, inc=1, device_id=(s, other), device_id_type=MESH)
    loop(
        1,
        sp_count,
        lambda i: pl.semaphore_signal(
            barrier, inc=1, device_id=(partner(i), t), device_id_type=MESH
        ),
    )
    loads = [
        pltpu.make_async_copy(src, dst, load_sem.at[k])
        for k, (src, dst) in enumerate(zip(refs_in, refs_here))
    ]
    for copy in loads:
        copy.start()
    for copy in loads[:5]:
        copy.wait()

    def cols_of(q):
        return pl.ds(pl.multiple_of(q * width, width), width)

    with scope("prepare"):
        cols = cols_of(t)
        res_all = res[...].astype(jnp.float32)
        inv_rms = lax.rsqrt(jnp.mean(res_all * res_all, axis=1, keepdims=True) + NORM_EPS)
        moe_part[...] = (res[:, cols].astype(jnp.float32) * inv_rms * gain[:, cols]).astype(
            jnp.bfloat16
        )
        square = (tok_rows, tok_rows)
        down_at = lax.broadcasted_iota(jnp.int32, square, 0)
        over_at = lax.broadcasted_iota(jnp.int32, square, 1)

        def column(row):
            return jnp.sum(jnp.where(down_at == over_at, row, 0.0), axis=1, keepdims=True)

        cot_mine = cot[:, cols].astype(jnp.float32)
        scaled_first[...] = (column(weights[0:1, :]) * cot_mine).astype(jnp.bfloat16)
        scaled_second[...] = (column(weights[1:2, :]) * cot_mine).astype(jnp.bfloat16)
        experts = lax.broadcasted_iota(jnp.int32, (sp_count, tok_rows), 0)
        is_first = ids[0:1, :] == experts
        is_second = ids[1:2, :] == experts
        hits = (is_first | is_second).astype(jnp.float32).astype(jnp.bfloat16)
        earlier = (down_at < over_at).astype(jnp.float32).astype(jnp.bfloat16)
        ranks = jnp.dot(hits, earlier, preferred_element_type=jnp.float32)
        row_first = jnp.sum(jnp.where(is_first, ranks, 0.0), axis=0, keepdims=True)
        row_second = jnp.sum(jnp.where(is_second, ranks, 0.0), axis=0, keepdims=True)
        row_first = row_first + (ids[0:1, :] * cap).astype(jnp.float32)
        row_second = row_second + (ids[1:2, :] * cap).astype(jnp.float32)
        slots = lax.broadcasted_iota(jnp.int32, (cap, tok_rows), 0).astype(jnp.float32)

    def filled(target):
        base = (target * cap).astype(jnp.float32)
        first = jnp.where(row_first - base == slots, 1.0, 0.0)
        second = jnp.where(row_second - base == slots, 1.0, 0.0)
        rows = jnp.dot(
            (first + second).astype(jnp.bfloat16),
            moe_part[...],
            preferred_element_type=jnp.float32,
        ).astype(jnp.bfloat16)
        from_first = jnp.dot(
            first.astype(jnp.bfloat16), scaled_first[...], preferred_element_type=jnp.float32
        )
        from_second = jnp.dot(
            second.astype(jnp.bfloat16), scaled_second[...], preferred_element_type=jnp.float32
        )
        return rows, (from_first + from_second).astype(jnp.bfloat16)

    def quarter_of(source, q):
        return held.at[source, :, :, cols_of(q)]

    def first(i):
        target = partner(i)
        return remote(
            sending.at[target], quarter_of(s, t), send_sem.at[0], recv_sem.at[0, i], (target, t)
        )

    def passed(kind, i, q, to):
        block = quarter_of(partner(i), q)
        landing = recv_sem.at[min(kind, 2), i]
        return remote(block, block, send_sem.at[kind], landing, (s, to))

    def landed(i):
        source = partner(i)
        remote(
            sending.at[source],
            quarter_of(source, t),
            send_sem.at[0],
            recv_sem.at[0, i],
            (source, t),
        ).wait_recv()

    def pass_on(i):
        passed(1, i, t, across).start()
        passed(2, i, t, beside).start()

    def pass_back(i):
        passed(1, i, across, across).wait_recv()
        passed(3, i, across, beside).start()

    def all_of(like, sem):
        return remote(like, like, sem, sem, (s, beside))

    def complete(i):
        all_of(sending.at[pl.ds(0, 2)], recv_sem.at[2, i]).wait_recv()

    rows_own, cot_own = filled(s)
    held[s, 0, :, cols] = rows_own
    held[s, 1, :, cols] = cot_own
    with scope("barrier"):
        pl.semaphore_wait(barrier, sp_count + 1)
    pass_on(0)

    def send_one(i):
        target = partner(i)
        rows, values = filled(target)
        sending[target, 0] = rows
        sending[target, 1] = values
        first(i).start()

    early = min(5, sp_count)
    with scope("sends"):
        loop(1, early, send_one)

    for copy in loads[5:11]:
        copy.wait()
    with scope("forward"):
        block = rate_map.shape[1]
        lane_in = lax.rem(lax.broadcasted_iota(jnp.int32, (block, channels), 1), block)
        spread_out = lane_in == lax.broadcasted_iota(jnp.int32, (block, channels), 0)
        spread_out = spread_out.astype(jnp.float32).astype(jnp.bfloat16)
        wide = (channels, channels)
        same = lax.div(lax.broadcasted_iota(jnp.int32, wide, 0), block) == lax.div(
            lax.broadcasted_iota(jnp.int32, wide, 1), block
        )
        for k, blocks in enumerate((rate_map, input_map)):
            tiled = jnp.dot(
                blocks[...].reshape(channels, block),
                spread_out,
                preferred_element_type=jnp.float32,
            )
            maps[:, k * channels : (k + 1) * channels] = jnp.where(same, tiled, 0.0).astype(
                jnp.bfloat16
            )
        pre_values[...] = jnp.dot(conv[...], maps[...], preferred_element_type=jnp.float32)
        y = jnp.exp(-decay[...])
        soft = y * (1.0 - y * (0.5 - y * (1.0 / 3.0 - y * (0.25 - y * 0.2))))
        step = 16

        def forward(i):
            rows = pl.ds(pl.multiple_of(i * step, step), step)
            rate_gate = jax.nn.sigmoid(pre_values[rows, :channels])
            input_gate = jax.nn.sigmoid(pre_values[rows, channels:])
            log_keep = -RATE_SCALE * rate_gate * soft
            kept = jnp.exp(log_keep)
            spread = -2.0 * log_keep
            gone = one_less_exp(spread)
            norm_term = jnp.sqrt(gone)
            conv_values = conv[rows, :].astype(jnp.float32)
            prev_values = prev[rows, :].astype(jnp.float32)
            inner = input_gate * conv_values
            state_now = kept * prev_values + norm_term * inner
            v = gate[rows, :].astype(jnp.float32)
            root = 0.7978845608028654
            bent = jnp.tanh(root * (v + 0.044715 * v * v * v))
            gelu_value = 0.5 * v * (1.0 + bent)
            gelu_slope = 0.5 * (1.0 + bent) + 0.5 * v * (1.0 - bent * bent) * root * (
                1.0 + 3.0 * 0.044715 * v * v
            )
            tiny_side = spread < SERIES_EDGE
            series = jnp.where(
                tiny_side, 1.0 + 0.5 * spread, spread / jnp.where(tiny_side, 1.0, gone)
            )
            slope = 0.5 * jnp.sqrt(spread * series)
            branch_all[s, rows, :] = (state_now * gelu_value).astype(jnp.bfloat16)
            rate_factor[rows, :] = prev_values * kept * (-RATE_SCALE * soft) * rate_gate * (
                1.0 - rate_gate
            ) + inner * kept * kept * (1.0 - rate_gate) * slope
            input_factor[rows, :] = norm_term * conv_values * input_gate * (1.0 - input_gate)
            direct_factor[rows, :] = norm_term * input_gate
            gate_factor[rows, :] = state_now * gelu_slope
            gelu_values[rows, :] = gelu_value
            keep[rows, :] = kept

        loop(0, tok_rows // step, forward)

    for copy in loads[11:]:
        copy.wait()

    def to_beside(i, k):
        source = partner(i)
        q = beside if k == 0 else facing
        return remote(
            part.at[source, :, cols_of(q)],
            from_beside.at[k, source],
            back_send.at[k],
            back_recv.at[k, i],
            (s, beside),
        )

    def crossing(i):
        source = partner(i)
        return remote(
            to_across.at[source],
            from_across.at[source],
            back_send.at[2],
            back_recv.at[2, i],
            (s, across),
        )

    def homeward(i):
        source = partner(i)
        return remote(
            leaving.at[source],
            arrived.at[s],
            back_send.at[3],
            back_recv.at[3, i],
            (source, t),
        )

    def expert(i):
        complete(i)
        source = partner(i)
        rows_in = held[source, 0]
        gate_pre = jnp.dot(rows_in, gate_w[...], preferred_element_type=jnp.float32)
        up_pre = jnp.dot(rows_in, up_w[...], preferred_element_type=jnp.float32)
        d_hidden = lax.dot_general(
            held[source, 1], down_w[...], OVER_COLS, preferred_element_type=jnp.float32
        )
        gate_sig = jax.nn.sigmoid(gate_pre)
        gate_act = gate_pre * gate_sig
        up_back = (d_hidden * gate_act).astype(jnp.bfloat16)
        gate_back = (d_hidden * up_pre * gate_sig * (1.0 + gate_pre * (1.0 - gate_sig))).astype(
            jnp.bfloat16
        )
        hidden[source] = (gate_act * up_pre).astype(jnp.bfloat16)
        d_up[source] = up_back
        d_gate[source] = gate_back
        back = lax.dot_general(
            gate_back, gate_w[...], OVER_COLS, preferred_element_type=jnp.float32
        )
        back = back + lax.dot_general(
            up_back, up_w[...], OVER_COLS, preferred_element_type=jnp.float32
        )
        part[source] = back.astype(jnp.bfloat16)
        to_beside(i, 1).start()
        to_beside(i, 0).start()

    def cross(i, at_once):
        to_beside(i, 1).wait_recv()
        at = partner(i)
        total = part[at, :, cols_of(across)].astype(jnp.float32) + from_beside[1, at].astype(
            jnp.float32
        )
        to_across[at] = total.astype(jnp.bfloat16)
        if at_once:
            crossing(i).start()
        to_beside(i, 0).wait_recv()
        mine[at] = part[at, :, cols].astype(jnp.float32) + from_beside[0, at].astype(jnp.float32)

    def leave(i):
        crossing(i).wait_recv()
        at = partner(i)
        total = (mine[at] + from_across[at].astype(jnp.float32)).astype(jnp.bfloat16)
        if isinstance(i, int) and i == 0:
            arrived[s] = total
        else:
            leaving[at] = total
            homeward(i).start()

    own_branch = branch_all.at[s]

    def branch_copy(j):
        return remote(
            own_branch,
            own_branch,
            branch_send.at[0],
            branch_recv.at[j],
            (partner(2 * j), t),
        )

    def branch_landed(j):
        source = partner(2 * j)
        return remote(
            own_branch,
            branch_all.at[source],
            branch_send.at[0],
            branch_recv.at[j],
            (source, t),
        )

    def branch_twin(j):
        block = branch_all.at[partner(2 * j)]
        return remote(block, block, branch_send.at[1], branch_recv.at[0], (s_twin, t))

    near = 4
    stride = 3 if sp_count == 8 else 2
    lag = 3 - stride

    def turn(i):
        @pl.when((i >= 2) & (i < sp_count + 2))
        def _():
            with scope("expert"):
                expert(i - 2)

        @pl.when((i >= near + 2) & (i < sp_count + 2))
        def _():
            with scope("cross"):
                cross(i - 2, True)

        @pl.when(i == sp_count)
        def _():
            crossing(2).start()
            crossing(3).start()

        @pl.when(i >= near + 3)
        def _():
            with scope("leave"):
                leave(i - 3)

        @pl.when(i == near + 3)
        def _():
            leave(0)
            leave(1)

        @pl.when(i == sp_count + 1)
        def _():
            leave(2)
            leave(3)

        @pl.when((i >= 1) & (i < sp_count))
        def _():
            with scope("landed"):
                landed(i)
            pass_on(i)

        @pl.when(i == 1)
        def _():
            branch_twin(0).start()

        @pl.when((i >= 3) & (i <= stride * (half - 2) + lag) & (lax.rem(i - lag, stride) == 0))
        def _():
            branch_copy(lax.div(i - lag, stride)).start()

        @pl.when((i >= 1) & (i + early - 1 < sp_count))
        def _():
            send_one(i + early - 1)

        @pl.when(i == near + 1)
        def _():
            crossing(0).start()
            crossing(1).start()

        @pl.when((i >= 1) & (i < sp_count + 1))
        def _():
            with scope("pass_back"):
                pass_back(i - 1)

        @pl.when((i >= 2) & (i < near + 2))
        def _():
            with scope("cross"):
                cross(i - 2, False)

    loop(0, sp_count + 3, turn)

    def pass_branch(j):
        branch_landed(j).wait_recv()
        branch_twin(j).start()

    with scope("branch_pass"):
        loop(1, half - 1, pass_branch)

    def merged(values):
        return values.reshape(sp_count * cap, values.shape[2])

    def summed(left, right):
        if cap % 16 == 0:
            return lax.dot_general(
                merged(left), merged(right), OVER_ROWS, preferred_element_type=jnp.float32
            )
        total = None
        for source in range(sp_count):
            one = lax.dot_general(
                left[source], right[source], OVER_ROWS, preferred_element_type=jnp.float32
            )
            total = one if total is None else total + one
        return total

    tile = 256
    def rows_tile(k):
        at = pl.ds(pl.multiple_of(k * tile, tile), tile)
        rows = held[:, 0, :, at]
        gate_grad[at, :] = summed(rows, d_gate[...])
        up_grad[at, :] = summed(rows, d_up[...])

    def cot_tile(k):
        at = pl.ds(pl.multiple_of(k * tile, tile), tile)
        down_grad[:, at] = summed(hidden[...], held[:, 1, :, at])

    with scope("grads_rows"):
        loop(0, model_width // tile, rows_tile)

    lanes = lax.broadcasted_iota(jnp.int32, (tok_rows, cap), 1).astype(jnp.float32)
    slot_first, slot_second = column(row_first), column(row_second)

    def gather_rows(source):
        base = (source * cap).astype(jnp.float32)
        chosen = jnp.where(slot_first - base == lanes, 1.0, 0.0)
        chosen = chosen + jnp.where(slot_second - base == lanes, 1.0, 0.0)
        return jnp.dot(
            chosen.astype(jnp.bfloat16), arrived[source], preferred_element_type=jnp.float32
        )

    def add_in(i, total):
        source = partner(i)
        with scope("home"):
            remote(
                leaving.at[source],
                arrived.at[source],
                back_send.at[3],
                back_recv.at[3, i],
                (source, t),
            ).wait_recv()
        return total + gather_rows(source)

    full[:, cols] = lax.fori_loop(1, sp_count, add_in, gather_rows(s)).astype(jnp.bfloat16)

    pair, other_pair = lax.div(t, 2), lax.div(across, 2)

    def gathered(kind, part_of, q, to, late):
        rows = pl.ds(pl.multiple_of(part_of * 2 * share_rows, 2 * share_rows), 2 * share_rows)
        block = full.at[rows, cols_of(q)]
        return remote(block, block, last_send.at[kind, late], last_recv.at[kind, late], (s, to))

    gathered(0, other_pair, t, across, 0).start()
    gathered(1, pair, t, beside, 0).start()
    gathered(0, pair, t, across, 1).start()
    gathered(1, other_pair, t, beside, 1).start()
    branch_copy(half - 1).start()
    with scope("grads_cot"):
        loop(0, model_width // tile, cot_tile)
    with scope("quarter"):
        gathered(0, pair, across, across, 0).wait_recv()
        gathered(2, pair, across, beside, 0).start()
        gathered(1, pair, beside, beside, 0).wait_recv()
        gathered(2, pair, facing, beside, 0).wait_recv()

    def mix_rows(begin):
        rows = pl.ds(pl.multiple_of(begin, share_rows), share_rows)
        values = res[rows, :].astype(jnp.float32)
        weighted = gain[...] * full[rows, :].astype(jnp.float32)
        inverse = lax.rsqrt(jnp.mean(values * values, axis=1, keepdims=True) + NORM_EPS)
        cubed = inverse * inverse * inverse
        slope = cubed * jnp.mean(values * weighted, axis=1, keepdims=True)
        return rows, (
            cot[rows, :].astype(jnp.float32) + inverse * weighted - values * slope
        ).astype(jnp.bfloat16)

    def share_view(source, q):
        return mix_all.at[source, pl.ds(pl.multiple_of(q * share_rows, share_rows), share_rows), :]

    def share_first(i):
        target = partner(i)
        return remote(
            share.at[target],
            share_view(s, t),
            share_send.at[0],
            share_recv.at[0, i],
            (target, t),
        )

    def share_passed(kind, i, q, to):
        block = share_view(partner(i), q)
        landing = share_recv.at[1, i] if kind == 1 else share_recv.at[0, 0]
        return remote(block, block, share_send.at[kind], landing, (s, to))

    def share_landed(i):
        source = partner(i)
        remote(
            share.at[source],
            share_view(source, t),
            share_send.at[0],
            share_recv.at[0, i],
            (source, t),
        ).wait_recv()

    def share_on(i):
        share_passed(1, i, t, across).start()
        share_passed(2, i, t, beside).start()

    def share_back(i):
        share_passed(1, i, across, across).wait_recv()
        share_passed(3, i, across, beside).start()

    with scope("share"):
        _, own_rows = mix_rows(t * share_rows)
        for j in range(sp_count):
            share[j] = own_rows[:, j * out_rows : (j + 1) * out_rows]
        loop(1, sp_count, lambda i: share_first(sp_count - i).start())
        own_at = pl.ds(pl.multiple_of(t * share_rows, share_rows), share_rows)
        mix_all[s, own_at, :] = share[s]
        share_on(0)

    with scope("quarter_late"):
        gathered(0, other_pair, across, across, 1).wait_recv()
        gathered(2, other_pair, across, beside, 1).start()
        gathered(1, other_pair, beside, beside, 1).wait_recv()
        gathered(2, other_pair, facing, beside, 1).wait_recv()

    with scope("mix"):

        def fill(k):
            rows, values = mix_rows(k * share_rows)
            mix[rows, :] = values

        loop(0, tp_count, fill)

    with scope("scan"):
        d_branch = jnp.dot(mix[...], proj[...], preferred_element_type=jnp.float32)
        branch_grad[...] = d_branch * gate_factor[...]
        at = lax.broadcasted_iota(jnp.int32, d_branch.shape, 0)
        grads = d_branch * gelu_values[...]
        keeps = jnp.where(at < tok_rows - 1, pltpu.roll(keep[...], tok_rows - 1, 0), 1.0)
        reach = 1
        while reach < tok_rows:
            inside = at < tok_rows - reach
            later_grads = jnp.where(inside, pltpu.roll(grads, tok_rows - reach, 0), 0.0)
            later_keeps = jnp.where(inside, pltpu.roll(keeps, tok_rows - reach, 0), 1.0)
            grads = grads + keeps * later_grads
            keeps = keeps * later_keeps
            reach *= 2
        small[...] = jnp.zeros_like(small)
        small[0:1, :] = keep[0:1, :] * keeps[0:1, :]
        small[1:2, :] = keep[0:1, :] * grads[0:1, :]
        small_all[s] = jnp.zeros(small.shape, jnp.float32)

    def carry_to(i):
        return remote(
            small, small_all.at[s], small_send.at[0], small_recv.at[0], (partner(i), t)
        )

    loop(1, sp_count, lambda i: carry_to(i).start())

    with scope("branch_last"):
        pass_branch(half - 1)

    def relay(i):
        @pl.when(i < sp_count)
        def _():
            share_landed(i)
            share_on(i)

        @pl.when(i >= 2)
        def _():
            share_back(i - 2)

    with scope("relay"):
        loop(1, sp_count + 2, relay)

    with scope("small"):
        all_of(small_all.at[pl.ds(0, sp_count - 1)], small_recv.at[0]).wait_recv()

    def compose(turn, carried):
        source = sp_count - 1 - turn
        later = small_all[source]
        return jnp.where(source > s, later[1:2] + later[0:1] * carried, carried)

    with scope("back_maps"):
        carried = lax.fori_loop(0, sp_count - 1, compose, jnp.zeros((1, channels), jnp.float32))
        state_grad = grads + keeps * carried
        back = jnp.concatenate(
            [state_grad * rate_factor[...], state_grad * input_factor[...]], axis=1
        )
        high = back.astype(jnp.bfloat16)
        low = (back - high.astype(jnp.float32)).astype(jnp.bfloat16)
        conv_grad[...] = (
            state_grad * direct_factor[...]
            + lax.dot_general(high, maps[...], OVER_COLS, preferred_element_type=jnp.float32)
            + lax.dot_general(low, maps[...], OVER_COLS, preferred_element_type=jnp.float32)
        )

    with scope("last_waits"):

        all_of(mix_all.at[:, pl.ds(0, 2 * share_rows)], share_recv.at[0, 0]).wait_recv()
        all_of(branch_all.at[pl.ds(0, half)], branch_recv.at[0]).wait_recv()
    with scope("grad_proj"):
        proj_grad[...] = lax.dot_general(
            mix_all[...].reshape(sp_count * tok_rows, out_rows),
            branch_all[...].reshape(sp_count * tok_rows, channels),
            OVER_ROWS,
            preferred_element_type=jnp.float32,
        )

    others = pl.ds(0, sp_count - 1)
    with scope("end"):
        all_of(sending.at[others], send_sem.at[0]).wait_send()
        for kind in (1, 2, 3):
            all_of(sending, send_sem.at[kind]).wait_send()
            all_of(to_across, back_send.at[kind - 1]).wait_send()
            all_of(share, share_send.at[kind]).wait_send()
        all_of(to_across.at[others], back_send.at[3]).wait_send()
        all_of(share.at[others], share_send.at[0]).wait_send()
        all_of(small_all.at[others], small_send.at[0]).wait_send()
        all_of(branch_all.at[pl.ds(0, half - 1)], branch_send.at[0]).wait_send()
        all_of(branch_all.at[pl.ds(0, half)], branch_send.at[1]).wait_send()
        for late, (near_half, far_half) in enumerate(((pair, other_pair), (other_pair, pair))):
            gathered(0, far_half, t, across, late).wait_send()
            gathered(1, near_half, t, beside, late).wait_send()
            gathered(2, near_half, across, beside, late).wait_send()


def layer(sp_count, tp_count, cap, operands):
    res, conv, gate_w, down_w = (operands[k] for k in (0, 5, 11, 13))
    tok_rows, model_width = res.shape
    channels, units = conv.shape[1], down_w.shape[0]
    width = model_width // tp_count
    share_rows, out_rows = tok_rows // tp_count, model_width // sp_count
    vmem = pl.BlockSpec(memory_space=pltpu.VMEM)
    anywhere = pl.BlockSpec(memory_space=pl.ANY)
    low, exact = jnp.bfloat16, jnp.float32
    blocks = (sp_count, cap, width)
    scratch = [
        ((channels, 2 * channels), low),
        ((sp_count, 2, cap, width), low),
        ((tok_rows, width), low),
        ((tok_rows, width), low),
        ((tok_rows, width), low),
        ((tok_rows, 2 * channels), exact),
        ((sp_count, 2, cap, model_width), low),
        ((sp_count, cap, model_width), low),
        ((2,) + blocks, low),
        (blocks, low),
        (blocks, low),
        (blocks, exact),
        (blocks, low),
        (blocks, low),
        (res.shape, low),
        ((sp_count, cap, units), low),
        ((sp_count, cap, units), low),
        ((sp_count, cap, units), low),
    ]
    scratch += [(conv.shape, exact)] * 6
    scratch += [
        ((sp_count,) + conv.shape, low),
        (res.shape, low),
        ((sp_count, share_rows, out_rows), low),
        ((sp_count, tok_rows, out_rows), low),
        ((8, channels), exact),
        ((sp_count, 8, channels), exact),
    ]
    sems = [
        (len(operands),),
        (4,),
        (3, sp_count),
        (4,),
        (4, sp_count),
        (2,),
        (sp_count // 2,),
        (3, 2),
        (3, 2),
        (4,),
        (2, sp_count),
        (1,),
        (1,),
    ]
    def grouped(*refs):
        layer_kernel(sp_count, tp_count, refs[: len(operands)], *refs[len(operands) :])

    return pl.pallas_call(
        grouped,
        out_shape=[
            pltpu.VMEM(shape, exact)
            for shape in (
                gate_w.shape,
                gate_w.shape,
                down_w.shape,
                (out_rows, channels),
                conv.shape,
                conv.shape,
            )
        ],
        in_specs=[anywhere] * len(operands),
        out_specs=[vmem] * 6,
        scratch_shapes=[[pltpu.VMEM(given.shape, given.dtype) for given in operands]]
        + [pltpu.VMEM(shape, kind) for shape, kind in scratch]
        + [pltpu.SemaphoreType.DMA(shape) for shape in sems],
        compiler_params=pltpu.CompilerParams(collective_id=1, has_side_effects=True, vmem_limit_bytes=59_000_000),
        cost_estimate=pl.CostEstimate(flops=0, bytes_accessed=40_000_000, transcendentals=0),
    )(*operands)


def store_kernel(*refs):
    count = len(refs) // 2
    sems = refs[-1]
    copies = [
        pltpu.make_async_copy(refs[k], refs[count + k], sems.at[k]) for k in range(count)
    ]
    for copy in copies:
        copy.start()
    for copy in copies:
        copy.wait()


def store(values):
    return pl.pallas_call(
        store_kernel,
        out_shape=[jax.ShapeDtypeStruct(value.shape, value.dtype) for value in values],
        in_specs=[pl.BlockSpec(memory_space=pltpu.VMEM)] * len(values),
        out_specs=[pl.BlockSpec(memory_space=pl.ANY)] * len(values),
        scratch_shapes=[pltpu.SemaphoreType.DMA((len(values),))],
        compiler_params=pltpu.CompilerParams(vmem_limit_bytes=16 * 1024 * 1024),
    )(*[pltpu.with_memory_space_constraint(value, pltpu.VMEM) for value in values])


def per_device(
    cotangent,
    residual,
    norm_gain,
    route_ids,
    route_weights,
    expert_gate,
    expert_up,
    expert_down,
    out_proj,
    conv_out,
    branch_gate,
    prev_state,
    decay_param,
    rate_map,
    input_map,
):
    sp_count = lax.axis_size("sp")
    tp_count = lax.axis_size("tp")
    experts_all = expert_gate.shape[0] * sp_count
    capacity = 4 * residual.shape[0] // experts_all
    grads = layer(
        sp_count,
        tp_count,
        capacity,
        (
            residual,
            cotangent,
            norm_gain[None, :],
            route_ids.T,
            route_weights.T,
            conv_out,
            branch_gate,
            prev_state,
            decay_param[None, :],
            rate_map,
            input_map,
            expert_gate[0],
            expert_up[0],
            expert_down[0],
            out_proj,
        ),
    )
    grad_gate, grad_up, grad_down, grad_out_proj, grad_conv_out, grad_branch_gate = store(grads)
    return (
        grad_gate[None],
        grad_up[None],
        grad_down[None],
        grad_out_proj,
        grad_conv_out,
        grad_branch_gate,
    )


def solution(mesh):
    in_specs = (
        P("sp", None),
        P("sp", None),
        P(),
        P("sp", None),
        P("sp", None),
        P("sp", None, "tp"),
        P("sp", None, "tp"),
        P("sp", "tp", None),
        P(None, "tp"),
        P("sp", "tp"),
        P("sp", "tp"),
        P("sp", "tp"),
        P("tp"),
        P("tp", None, None),
        P("tp", None, None),
    )
    out_specs = (
        P("sp", None, "tp"),
        P("sp", None, "tp"),
        P("sp", "tp", None),
        P("sp", "tp"),
        P("sp", "tp"),
        P("sp", "tp"),
    )
    return jax.shard_map(
        per_device, mesh=mesh, in_specs=in_specs, out_specs=out_specs, check_vma=False
    )
```

```python
import contextlib

import jax
import jax.numpy as jnp
from jax import lax
from jax.sharding import PartitionSpec as P
from jax.experimental import pallas as pl
from jax.experimental.pallas import tpu as pltpu

RATE_SCALE = 8.0
NORM_EPS = 1e-06
SERIES_EDGE = 0.001
MESH = pl.DeviceIdType.MESH
SCOPES = False
OVER_ROWS = (((0,), (0,)), ((), ()))
OVER_COLS = (((1,), (1,)), ((), ()))


def scope(name):
    return jax.named_scope(name) if SCOPES else contextlib.nullcontext()


def partner_of(place, i, count):
    total = lax.rem(place + i, 2)
    bit = 2
    while bit < count:
        own = lax.div(place, bit) + lax.div(i, bit) + lax.div(i, 2 * bit)
        total = total + bit * lax.rem(own, 2)
        bit *= 2
    return total


def remote(src, dst, send_sem, recv_sem, device):
    return pltpu.make_async_remote_copy(
        src_ref=src,
        dst_ref=dst,
        send_sem=send_sem,
        recv_sem=recv_sem,
        device_id=device,
        device_id_type=MESH,
    )


def one_less_exp(spread):
    small = jnp.minimum(spread, 0.3)
    series = jnp.full_like(small, 1.0 / 40320.0)
    for factorial in (5040.0, 720.0, 120.0, 24.0, 6.0, 2.0, 1.0):
        series = 1.0 / factorial - small * series
    return jnp.where(spread < 0.3, small * series, 1.0 - jnp.exp(-spread))


def loop(begin, end, step):
    def body(i, carry):
        step(i)
        return carry

    lax.fori_loop(begin, end, body, 0)


def layer_kernel(
    sp_count,
    tp_count,
    refs_in,
    gate_grad,
    up_grad,
    down_grad,
    proj_grad,
    conv_grad,
    branch_grad,
    refs_here,
    maps,
    sending,
    moe_part,
    scaled_first,
    scaled_second,
    pre_values,
    held,
    part,
    from_beside,
    to_across,
    from_across,
    mine,
    leaving,
    arrived,
    full,
    hidden,
    d_gate,
    d_up,
    rate_factor,
    input_factor,
    direct_factor,
    gate_factor,
    gelu_values,
    keep,
    branch_all,
    mix,
    share,
    mix_all,
    small,
    small_all,
    load_sem,
    send_sem,
    recv_sem,
    back_send,
    back_recv,
    branch_send,
    branch_recv,
    last_send,
    last_recv,
    share_send,
    share_recv,
    small_send,
    small_recv,
):
    s = lax.axis_index("sp")
    t = lax.axis_index("tp")
    beside = t + 1 - 2 * lax.rem(t, 2)
    across = lax.rem(t + tp_count // 2, tp_count)
    facing = lax.rem(beside + tp_count // 2, tp_count)
    half = sp_count // 2
    s_twin = s + 1 - 2 * lax.rem(s, 2)
    (res, cot, gain, ids, weights, conv, gate, prev, decay, rate_map, input_map) = refs_here[:11]
    gate_w, up_w, down_w, proj = refs_here[11:]
    tok_rows, model_width = res.shape
    cap, width = sending.shape[2:]
    channels = conv.shape[1]
    share_rows, out_rows = share.shape[1:]

    def partner(i):
        return partner_of(s, i, sp_count)

    barrier = pltpu.get_barrier_semaphore()
    for other in (beside, across):
        pl.semaphore_signal(barrier, inc=1, device_id=(s, other), device_id_type=MESH)
    loop(
        1,
        sp_count,
        lambda i: pl.semaphore_signal(
            barrier, inc=1, device_id=(partner(i), t), device_id_type=MESH
        ),
    )
    loads = [
        pltpu.make_async_copy(src, dst, load_sem.at[k])
        for k, (src, dst) in enumerate(zip(refs_in, refs_here))
    ]
    for copy in loads:
        copy.start()
    for copy in loads[:5]:
        copy.wait()

    def cols_of(q):
        return pl.ds(pl.multiple_of(q * width, width), width)

    with scope("prepare"):
        cols = cols_of(t)
        res_all = res[...].astype(jnp.float32)
        inv_rms = lax.rsqrt(jnp.mean(res_all * res_all, axis=1, keepdims=True) + NORM_EPS)
        moe_part[...] = (res[:, cols].astype(jnp.float32) * inv_rms * gain[:, cols]).astype(
            jnp.bfloat16
        )
        square = (tok_rows, tok_rows)
        down_at = lax.broadcasted_iota(jnp.int32, square, 0)
        over_at = lax.broadcasted_iota(jnp.int32, square, 1)

        def column(row):
            return jnp.sum(jnp.where(down_at == over_at, row, 0.0), axis=1, keepdims=True)

        cot_mine = cot[:, cols].astype(jnp.float32)
        scaled_first[...] = (column(weights[0:1, :]) * cot_mine).astype(jnp.bfloat16)
        scaled_second[...] = (column(weights[1:2, :]) * cot_mine).astype(jnp.bfloat16)
        experts = lax.broadcasted_iota(jnp.int32, (sp_count, tok_rows), 0)
        is_first = ids[0:1, :] == experts
        is_second = ids[1:2, :] == experts
        hits = (is_first | is_second).astype(jnp.float32).astype(jnp.bfloat16)
        earlier = (down_at < over_at).astype(jnp.float32).astype(jnp.bfloat16)
        ranks = jnp.dot(hits, earlier, preferred_element_type=jnp.float32)
        row_first = jnp.sum(jnp.where(is_first, ranks, 0.0), axis=0, keepdims=True)
        row_second = jnp.sum(jnp.where(is_second, ranks, 0.0), axis=0, keepdims=True)
        row_first = row_first + (ids[0:1, :] * cap).astype(jnp.float32)
        row_second = row_second + (ids[1:2, :] * cap).astype(jnp.float32)
        slots = lax.broadcasted_iota(jnp.int32, (cap, tok_rows), 0).astype(jnp.float32)

    def filled(target):
        base = (target * cap).astype(jnp.float32)
        first = jnp.where(row_first - base == slots, 1.0, 0.0)
        second = jnp.where(row_second - base == slots, 1.0, 0.0)
        rows = jnp.dot(
            (first + second).astype(jnp.bfloat16),
            moe_part[...],
            preferred_element_type=jnp.float32,
        ).astype(jnp.bfloat16)
        from_first = jnp.dot(
            first.astype(jnp.bfloat16), scaled_first[...], preferred_element_type=jnp.float32
        )
        from_second = jnp.dot(
            second.astype(jnp.bfloat16), scaled_second[...], preferred_element_type=jnp.float32
        )
        return rows, (from_first + from_second).astype(jnp.bfloat16)

    def quarter_of(source, q):
        return held.at[source, :, :, cols_of(q)]

    def first(i):
        target = partner(i)
        return remote(
            sending.at[target], quarter_of(s, t), send_sem.at[0], recv_sem.at[0, i], (target, t)
        )

    def passed(kind, i, q, to):
        block = quarter_of(partner(i), q)
        landing = recv_sem.at[min(kind, 2), i]
        return remote(block, block, send_sem.at[kind], landing, (s, to))

    def landed(i):
        source = partner(i)
        remote(
            sending.at[source],
            quarter_of(source, t),
            send_sem.at[0],
            recv_sem.at[0, i],
            (source, t),
        ).wait_recv()

    def pass_on(i):
        passed(1, i, t, across).start()
        passed(2, i, t, beside).start()

    def pass_back(i):
        passed(1, i, across, across).wait_recv()
        passed(3, i, across, beside).start()

    def all_of(like, sem):
        return remote(like, like, sem, sem, (s, beside))

    def complete(i):
        all_of(sending.at[pl.ds(0, 2)], recv_sem.at[2, i]).wait_recv()

    rows_own, cot_own = filled(s)
    held[s, 0, :, cols] = rows_own
    held[s, 1, :, cols] = cot_own
    with scope("barrier"):
        pl.semaphore_wait(barrier, sp_count + 1)
    pass_on(0)

    def send_one(i):
        target = partner(i)
        rows, values = filled(target)
        sending[target, 0] = rows
        sending[target, 1] = values
        first(i).start()

    early = min(5, sp_count)
    with scope("sends"):
        loop(1, early, send_one)

    for copy in loads[5:11]:
        copy.wait()
    with scope("forward"):
        block = rate_map.shape[1]
        lane_in = lax.rem(lax.broadcasted_iota(jnp.int32, (block, channels), 1), block)
        spread_out = lane_in == lax.broadcasted_iota(jnp.int32, (block, channels), 0)
        spread_out = spread_out.astype(jnp.float32).astype(jnp.bfloat16)
        wide = (channels, channels)
        same = lax.div(lax.broadcasted_iota(jnp.int32, wide, 0), block) == lax.div(
            lax.broadcasted_iota(jnp.int32, wide, 1), block
        )
        for k, blocks in enumerate((rate_map, input_map)):
            tiled = jnp.dot(
                blocks[...].reshape(channels, block),
                spread_out,
                preferred_element_type=jnp.float32,
            )
            maps[:, k * channels : (k + 1) * channels] = jnp.where(same, tiled, 0.0).astype(
                jnp.bfloat16
            )
        pre_values[...] = jnp.dot(conv[...], maps[...], preferred_element_type=jnp.float32)
        y = jnp.exp(-decay[...])
        soft = y * (1.0 - y * (0.5 - y * (1.0 / 3.0 - y * (0.25 - y * 0.2))))
        step = 16

        def forward(i):
            rows = pl.ds(pl.multiple_of(i * step, step), step)
            rate_gate = jax.nn.sigmoid(pre_values[rows, :channels])
            input_gate = jax.nn.sigmoid(pre_values[rows, channels:])
            log_keep = -RATE_SCALE * rate_gate * soft
            kept = jnp.exp(log_keep)
            spread = -2.0 * log_keep
            gone = one_less_exp(spread)
            norm_term = jnp.sqrt(gone)
            conv_values = conv[rows, :].astype(jnp.float32)
            prev_values = prev[rows, :].astype(jnp.float32)
            inner = input_gate * conv_values
            state_now = kept * prev_values + norm_term * inner
            v = gate[rows, :].astype(jnp.float32)
            root = 0.7978845608028654
            bent = jnp.tanh(root * (v + 0.044715 * v * v * v))
            gelu_value = 0.5 * v * (1.0 + bent)
            gelu_slope = 0.5 * (1.0 + bent) + 0.5 * v * (1.0 - bent * bent) * root * (
                1.0 + 3.0 * 0.044715 * v * v
            )
            tiny_side = spread < SERIES_EDGE
            series = jnp.where(
                tiny_side, 1.0 + 0.5 * spread, spread / jnp.where(tiny_side, 1.0, gone)
            )
            slope = 0.5 * jnp.sqrt(spread * series)
            branch_all[s, rows, :] = (state_now * gelu_value).astype(jnp.bfloat16)
            rate_factor[rows, :] = prev_values * kept * (-RATE_SCALE * soft) * rate_gate * (
                1.0 - rate_gate
            ) + inner * kept * kept * (1.0 - rate_gate) * slope
            input_factor[rows, :] = norm_term * conv_values * input_gate * (1.0 - input_gate)
            direct_factor[rows, :] = norm_term * input_gate
            gate_factor[rows, :] = state_now * gelu_slope
            gelu_values[rows, :] = gelu_value
            keep[rows, :] = kept

        loop(0, tok_rows // step, forward)

    for copy in loads[11:]:
        copy.wait()

    def to_beside(i, k):
        source = partner(i)
        q = beside if k == 0 else facing
        return remote(
            part.at[source, :, cols_of(q)],
            from_beside.at[k, source],
            back_send.at[k],
            back_recv.at[k, i],
            (s, beside),
        )

    def crossing(i):
        source = partner(i)
        return remote(
            to_across.at[source],
            from_across.at[source],
            back_send.at[2],
            back_recv.at[2, i],
            (s, across),
        )

    def homeward(i):
        source = partner(i)
        return remote(
            leaving.at[source],
            arrived.at[s],
            back_send.at[3],
            back_recv.at[3, i],
            (source, t),
        )

    def expert(i):
        complete(i)
        source = partner(i)
        rows_in = held[source, 0]
        gate_pre = jnp.dot(rows_in, gate_w[...], preferred_element_type=jnp.float32)
        up_pre = jnp.dot(rows_in, up_w[...], preferred_element_type=jnp.float32)
        d_hidden = lax.dot_general(
            held[source, 1], down_w[...], OVER_COLS, preferred_element_type=jnp.float32
        )
        gate_sig = jax.nn.sigmoid(gate_pre)
        gate_act = gate_pre * gate_sig
        up_back = (d_hidden * gate_act).astype(jnp.bfloat16)
        gate_back = (d_hidden * up_pre * gate_sig * (1.0 + gate_pre * (1.0 - gate_sig))).astype(
            jnp.bfloat16
        )
        hidden[source] = (gate_act * up_pre).astype(jnp.bfloat16)
        d_up[source] = up_back
        d_gate[source] = gate_back
        back = lax.dot_general(
            gate_back, gate_w[...], OVER_COLS, preferred_element_type=jnp.float32
        )
        back = back + lax.dot_general(
            up_back, up_w[...], OVER_COLS, preferred_element_type=jnp.float32
        )
        part[source] = back.astype(jnp.bfloat16)
        to_beside(i, 1).start()
        to_beside(i, 0).start()

    def cross(i, at_once):
        to_beside(i, 1).wait_recv()
        at = partner(i)
        total = part[at, :, cols_of(across)].astype(jnp.float32) + from_beside[1, at].astype(
            jnp.float32
        )
        to_across[at] = total.astype(jnp.bfloat16)
        if at_once:
            crossing(i).start()
        to_beside(i, 0).wait_recv()
        mine[at] = part[at, :, cols].astype(jnp.float32) + from_beside[0, at].astype(jnp.float32)

    def leave(i):
        crossing(i).wait_recv()
        at = partner(i)
        total = (mine[at] + from_across[at].astype(jnp.float32)).astype(jnp.bfloat16)
        if isinstance(i, int) and i == 0:
            arrived[s] = total
        else:
            leaving[at] = total
            homeward(i).start()

    own_branch = branch_all.at[s]

    def branch_copy(j):
        return remote(
            own_branch,
            own_branch,
            branch_send.at[0],
            branch_recv.at[j],
            (partner(2 * j), t),
        )

    def branch_landed(j):
        source = partner(2 * j)
        return remote(
            own_branch,
            branch_all.at[source],
            branch_send.at[0],
            branch_recv.at[j],
            (source, t),
        )

    def branch_twin(j):
        block = branch_all.at[partner(2 * j)]
        return remote(block, block, branch_send.at[1], branch_recv.at[0], (s_twin, t))

    near = 4
    stride = 3 if sp_count == 8 else 2
    lag = 3 - stride

    def turn(i):
        @pl.when((i >= 2) & (i < sp_count + 2))
        def _():
            with scope("expert"):
                expert(i - 2)

        @pl.when((i >= near + 2) & (i < sp_count + 2))
        def _():
            with scope("cross"):
                cross(i - 2, True)

        @pl.when(i == sp_count)
        def _():
            crossing(2).start()
            crossing(3).start()

        @pl.when(i >= near + 3)
        def _():
            with scope("leave"):
                leave(i - 3)

        @pl.when(i == near + 3)
        def _():
            leave(0)
            leave(1)

        @pl.when(i == sp_count + 1)
        def _():
            leave(2)
            leave(3)

        @pl.when((i >= 1) & (i < sp_count))
        def _():
            with scope("landed"):
                landed(i)
            pass_on(i)

        @pl.when(i == 1)
        def _():
            branch_twin(0).start()

        @pl.when((i >= 3) & (i <= stride * (half - 2) + lag) & (lax.rem(i - lag, stride) == 0))
        def _():
            branch_copy(lax.div(i - lag, stride)).start()

        @pl.when((i >= 1) & (i + early - 1 < sp_count))
        def _():
            send_one(i + early - 1)

        @pl.when(i == near + 1)
        def _():
            crossing(0).start()
            crossing(1).start()

        @pl.when((i >= 1) & (i < sp_count + 1))
        def _():
            with scope("pass_back"):
                pass_back(i - 1)

        @pl.when((i >= 2) & (i < near + 2))
        def _():
            with scope("cross"):
                cross(i - 2, False)

    loop(0, sp_count + 3, turn)

    def pass_branch(j):
        branch_landed(j).wait_recv()
        branch_twin(j).start()

    with scope("branch_pass"):
        loop(1, half - 1, pass_branch)

    def merged(values):
        return values.reshape(sp_count * cap, values.shape[2])

    def summed(left, right):
        if cap % 16 == 0:
            return lax.dot_general(
                merged(left), merged(right), OVER_ROWS, preferred_element_type=jnp.float32
            )
        total = None
        for source in range(sp_count):
            one = lax.dot_general(
                left[source], right[source], OVER_ROWS, preferred_element_type=jnp.float32
            )
            total = one if total is None else total + one
        return total

    tile = 256
    def rows_tile(k):
        at = pl.ds(pl.multiple_of(k * tile, tile), tile)
        rows = held[:, 0, :, at]
        gate_grad[at, :] = summed(rows, d_gate[...])
        up_grad[at, :] = summed(rows, d_up[...])

    def cot_tile(k):
        at = pl.ds(pl.multiple_of(k * tile, tile), tile)
        down_grad[:, at] = summed(hidden[...], held[:, 1, :, at])

    with scope("grads_rows"):
        loop(0, model_width // tile, rows_tile)

    lanes = lax.broadcasted_iota(jnp.int32, (tok_rows, cap), 1).astype(jnp.float32)
    slot_first, slot_second = column(row_first), column(row_second)

    def gather_rows(source):
        base = (source * cap).astype(jnp.float32)
        chosen = jnp.where(slot_first - base == lanes, 1.0, 0.0)
        chosen = chosen + jnp.where(slot_second - base == lanes, 1.0, 0.0)
        return jnp.dot(
            chosen.astype(jnp.bfloat16), arrived[source], preferred_element_type=jnp.float32
        )

    def add_in(i, total):
        source = partner(i)
        with scope("home"):
            remote(
                leaving.at[source],
                arrived.at[source],
                back_send.at[3],
                back_recv.at[3, i],
                (source, t),
            ).wait_recv()
        return total + gather_rows(source)

    full[:, cols] = lax.fori_loop(1, sp_count, add_in, gather_rows(s)).astype(jnp.bfloat16)

    pair, other_pair = lax.div(t, 2), lax.div(across, 2)

    def rows_of(q):
        return pl.ds(pl.multiple_of(q * share_rows, share_rows), share_rows)

    def pair_rows(p):
        return pl.ds(pl.multiple_of(p * 2 * share_rows, 2 * share_rows), 2 * share_rows)

    def given(kind, rows, q, to):
        block = full.at[rows, cols_of(q)]
        return remote(block, block, last_send.at[kind], last_recv.at[kind], (s, to))

    def own_first(kind, mine_too):
        peer = (across, beside, facing)[kind]
        return given(kind, rows_of(t), peer, peer) if mine_too else given(kind, rows_of(peer), t, peer)

    for kind in (2, 0, 1):
        own_first(kind, False).start()

    def rest_across(at_peer):
        if at_peer:
            return (
                given(3, pair_rows(other_pair), across, across),
                given(4, rows_of(beside), across, across),
            )
        return given(3, pair_rows(pair), t, across), given(4, rows_of(facing), t, across)

    def rest_beside(at_peer):
        if at_peer:
            return (
                given(5, pair_rows(other_pair), beside, beside),
                given(6, rows_of(beside), beside, beside),
            )
        return given(5, pair_rows(other_pair), t, beside), given(6, rows_of(t), t, beside)

    def rest_facing(at_peer):
        if at_peer:
            return (
                given(7, pair_rows(other_pair), facing, beside),
                given(8, rows_of(beside), facing, beside),
            )
        return given(7, pair_rows(other_pair), across, beside), given(8, rows_of(t), across, beside)

    for copy in rest_across(False) + rest_beside(False):
        copy.start()
    branch_copy(half - 1).start()
    with scope("grads_cot"):
        loop(0, model_width // tile, cot_tile)
    with scope("quarter"):
        for kind in range(3):
            own_first(kind, True).wait_recv()

    def mix_rows(begin):
        rows = pl.ds(pl.multiple_of(begin, share_rows), share_rows)
        values = res[rows, :].astype(jnp.float32)
        weighted = gain[...] * full[rows, :].astype(jnp.float32)
        inverse = lax.rsqrt(jnp.mean(values * values, axis=1, keepdims=True) + NORM_EPS)
        cubed = inverse * inverse * inverse
        slope = cubed * jnp.mean(values * weighted, axis=1, keepdims=True)
        return rows, (
            cot[rows, :].astype(jnp.float32) + inverse * weighted - values * slope
        ).astype(jnp.bfloat16)

    def share_view(source, q):
        return mix_all.at[source, pl.ds(pl.multiple_of(q * share_rows, share_rows), share_rows), :]

    def share_first(i):
        target = partner(i)
        return remote(
            share.at[target],
            share_view(s, t),
            share_send.at[0],
            share_recv.at[0, i],
            (target, t),
        )

    def share_passed(kind, i, q, to):
        block = share_view(partner(i), q)
        landing = share_recv.at[1, i] if kind == 1 else share_recv.at[0, 0]
        return remote(block, block, share_send.at[kind], landing, (s, to))

    def share_landed(i):
        source = partner(i)
        remote(
            share.at[source],
            share_view(source, t),
            share_send.at[0],
            share_recv.at[0, i],
            (source, t),
        ).wait_recv()

    straight = 5 * sp_count // 8

    def share_on(i):
        share_passed(1, i, t, across).start()

        @pl.when(i >= straight)
        def _():
            share_passed(3, i, t, facing).start()

        share_passed(2, i, t, beside).start()

    def share_back(i):
        share_passed(1, i, across, across).wait_recv()

        @pl.when(i < straight)
        def _():
            share_passed(3, i, across, beside).start()

    with scope("share"):
        _, own_rows = mix_rows(t * share_rows)
        for j in range(sp_count):
            share[j] = own_rows[:, j * out_rows : (j + 1) * out_rows]
        loop(1, sp_count, lambda i: share_first(sp_count - i).start())
        own_at = pl.ds(pl.multiple_of(t * share_rows, share_rows), share_rows)
        mix_all[s, own_at, :] = share[s]
        share_on(0)

    with scope("quarter_late"):
        for copy in rest_across(True):
            copy.wait_recv()
        for copy in rest_facing(False):
            copy.start()
        for copy in rest_beside(True) + rest_facing(True):
            copy.wait_recv()

    def relay(i):
        share_landed(i)
        share_on(i)

    with scope("relay"):
        loop(1, sp_count, relay)

    with scope("mix"):

        def fill(k):
            rows, values = mix_rows(k * share_rows)
            mix[rows, :] = values

        loop(0, tp_count, fill)

    with scope("scan"):
        d_branch = jnp.dot(mix[...], proj[...], preferred_element_type=jnp.float32)
        branch_grad[...] = d_branch * gate_factor[...]
        at = lax.broadcasted_iota(jnp.int32, d_branch.shape, 0)
        grads = d_branch * gelu_values[...]
        keeps = jnp.where(at < tok_rows - 1, pltpu.roll(keep[...], tok_rows - 1, 0), 1.0)
        reach = 1
        while reach < tok_rows:
            inside = at < tok_rows - reach
            later_grads = jnp.where(inside, pltpu.roll(grads, tok_rows - reach, 0), 0.0)
            later_keeps = jnp.where(inside, pltpu.roll(keeps, tok_rows - reach, 0), 1.0)
            grads = grads + keeps * later_grads
            keeps = keeps * later_keeps
            reach *= 2
        small[...] = jnp.zeros_like(small)
        small[0:1, :] = keep[0:1, :] * keeps[0:1, :]
        small[1:2, :] = keep[0:1, :] * grads[0:1, :]
        small_all[s] = jnp.zeros(small.shape, jnp.float32)

    def carry_to(i):
        return remote(
            small, small_all.at[s], small_send.at[0], small_recv.at[0], (partner(i), t)
        )

    loop(1, sp_count, lambda i: carry_to(i).start())

    with scope("branch_last"):
        pass_branch(half - 1)

    with scope("relay_back"):
        loop(0, sp_count, share_back)

    with scope("small"):
        all_of(small_all.at[pl.ds(0, sp_count - 1)], small_recv.at[0]).wait_recv()

    def compose(turn, carried):
        source = sp_count - 1 - turn
        later = small_all[source]
        return jnp.where(source > s, later[1:2] + later[0:1] * carried, carried)

    with scope("back_maps"):
        carried = lax.fori_loop(0, sp_count - 1, compose, jnp.zeros((1, channels), jnp.float32))
        state_grad = grads + keeps * carried
        back = jnp.concatenate(
            [state_grad * rate_factor[...], state_grad * input_factor[...]], axis=1
        )
        high = back.astype(jnp.bfloat16)
        low = (back - high.astype(jnp.float32)).astype(jnp.bfloat16)
        conv_grad[...] = (
            state_grad * direct_factor[...]
            + lax.dot_general(high, maps[...], OVER_COLS, preferred_element_type=jnp.float32)
            + lax.dot_general(low, maps[...], OVER_COLS, preferred_element_type=jnp.float32)
        )

    with scope("last_waits"):

        all_of(mix_all.at[:, pl.ds(0, 2 * share_rows)], share_recv.at[0, 0]).wait_recv()
        all_of(branch_all.at[pl.ds(0, half)], branch_recv.at[0]).wait_recv()
    with scope("grad_proj"):
        proj_grad[...] = lax.dot_general(
            mix_all[...].reshape(sp_count * tok_rows, out_rows),
            branch_all[...].reshape(sp_count * tok_rows, channels),
            OVER_ROWS,
            preferred_element_type=jnp.float32,
        )

    others = pl.ds(0, sp_count - 1)
    with scope("end"):
        all_of(sending.at[others], send_sem.at[0]).wait_send()
        for kind in (1, 2, 3):
            all_of(sending, send_sem.at[kind]).wait_send()
            all_of(to_across, back_send.at[kind - 1]).wait_send()
            all_of(share, share_send.at[kind]).wait_send()
        all_of(to_across.at[others], back_send.at[3]).wait_send()
        all_of(share.at[others], share_send.at[0]).wait_send()
        all_of(small_all.at[others], small_send.at[0]).wait_send()
        all_of(branch_all.at[pl.ds(0, half - 1)], branch_send.at[0]).wait_send()
        all_of(branch_all.at[pl.ds(0, half)], branch_send.at[1]).wait_send()
        for kind in range(3):
            own_first(kind, False).wait_send()
        for copy in rest_across(False) + rest_beside(False) + rest_facing(False):
            copy.wait_send()


def layer(sp_count, tp_count, cap, operands):
    res, conv, gate_w, down_w = (operands[k] for k in (0, 5, 11, 13))
    tok_rows, model_width = res.shape
    channels, units = conv.shape[1], down_w.shape[0]
    width = model_width // tp_count
    share_rows, out_rows = tok_rows // tp_count, model_width // sp_count
    vmem = pl.BlockSpec(memory_space=pltpu.VMEM)
    anywhere = pl.BlockSpec(memory_space=pl.ANY)
    low, exact = jnp.bfloat16, jnp.float32
    blocks = (sp_count, cap, width)
    scratch = [
        ((channels, 2 * channels), low),
        ((sp_count, 2, cap, width), low),
        ((tok_rows, width), low),
        ((tok_rows, width), low),
        ((tok_rows, width), low),
        ((tok_rows, 2 * channels), exact),
        ((sp_count, 2, cap, model_width), low),
        ((sp_count, cap, model_width), low),
        ((2,) + blocks, low),
        (blocks, low),
        (blocks, low),
        (blocks, exact),
        (blocks, low),
        (blocks, low),
        (res.shape, low),
        ((sp_count, cap, units), low),
        ((sp_count, cap, units), low),
        ((sp_count, cap, units), low),
    ]
    scratch += [(conv.shape, exact)] * 6
    scratch += [
        ((sp_count,) + conv.shape, low),
        (res.shape, low),
        ((sp_count, share_rows, out_rows), low),
        ((sp_count, tok_rows, out_rows), low),
        ((8, channels), exact),
        ((sp_count, 8, channels), exact),
    ]
    sems = [
        (len(operands),),
        (4,),
        (3, sp_count),
        (4,),
        (4, sp_count),
        (2,),
        (sp_count // 2,),
        (9,),
        (9,),
        (4,),
        (2, sp_count),
        (1,),
        (1,),
    ]
    def grouped(*refs):
        layer_kernel(sp_count, tp_count, refs[: len(operands)], *refs[len(operands) :])

    return pl.pallas_call(
        grouped,
        out_shape=[
            pltpu.VMEM(shape, exact)
            for shape in (
                gate_w.shape,
                gate_w.shape,
                down_w.shape,
                (out_rows, channels),
                conv.shape,
                conv.shape,
            )
        ],
        in_specs=[anywhere] * len(operands),
        out_specs=[vmem] * 6,
        scratch_shapes=[[pltpu.VMEM(given.shape, given.dtype) for given in operands]]
        + [pltpu.VMEM(shape, kind) for shape, kind in scratch]
        + [pltpu.SemaphoreType.DMA(shape) for shape in sems],
        compiler_params=pltpu.CompilerParams(collective_id=1, has_side_effects=True, vmem_limit_bytes=59_000_000),
        cost_estimate=pl.CostEstimate(flops=0, bytes_accessed=40_000_000, transcendentals=0),
    )(*operands)


def store_kernel(*refs):
    count = len(refs) // 2
    sems = refs[-1]
    copies = [
        pltpu.make_async_copy(refs[k], refs[count + k], sems.at[k]) for k in range(count)
    ]
    for copy in copies:
        copy.start()
    for copy in copies:
        copy.wait()


def store(values):
    return pl.pallas_call(
        store_kernel,
        out_shape=[jax.ShapeDtypeStruct(value.shape, value.dtype) for value in values],
        in_specs=[pl.BlockSpec(memory_space=pltpu.VMEM)] * len(values),
        out_specs=[pl.BlockSpec(memory_space=pl.ANY)] * len(values),
        scratch_shapes=[pltpu.SemaphoreType.DMA((len(values),))],
        compiler_params=pltpu.CompilerParams(vmem_limit_bytes=16 * 1024 * 1024),
    )(*[pltpu.with_memory_space_constraint(value, pltpu.VMEM) for value in values])


def per_device(
    cotangent,
    residual,
    norm_gain,
    route_ids,
    route_weights,
    expert_gate,
    expert_up,
    expert_down,
    out_proj,
    conv_out,
    branch_gate,
    prev_state,
    decay_param,
    rate_map,
    input_map,
):
    sp_count = lax.axis_size("sp")
    tp_count = lax.axis_size("tp")
    experts_all = expert_gate.shape[0] * sp_count
    capacity = 4 * residual.shape[0] // experts_all
    grads = layer(
        sp_count,
        tp_count,
        capacity,
        (
            residual,
            cotangent,
            norm_gain[None, :],
            route_ids.T,
            route_weights.T,
            conv_out,
            branch_gate,
            prev_state,
            decay_param[None, :],
            rate_map,
            input_map,
            expert_gate[0],
            expert_up[0],
            expert_down[0],
            out_proj,
        ),
    )
    grad_gate, grad_up, grad_down, grad_out_proj, grad_conv_out, grad_branch_gate = store(grads)
    return (
        grad_gate[None],
        grad_up[None],
        grad_down[None],
        grad_out_proj,
        grad_conv_out,
        grad_branch_gate,
    )


def solution(mesh):
    in_specs = (
        P("sp", None),
        P("sp", None),
        P(),
        P("sp", None),
        P("sp", None),
        P("sp", None, "tp"),
        P("sp", None, "tp"),
        P("sp", "tp", None),
        P(None, "tp"),
        P("sp", "tp"),
        P("sp", "tp"),
        P("sp", "tp"),
        P("tp"),
        P("tp", None, None),
        P("tp", None, None),
    )
    out_specs = (
        P("sp", None, "tp"),
        P("sp", None, "tp"),
        P("sp", "tp", None),
        P("sp", "tp"),
        P("sp", "tp"),
        P("sp", "tp"),
    )
    return jax.shard_map(
        per_device, mesh=mesh, in_specs=in_specs, out_specs=out_specs, check_vma=False
    )
```

```python
import contextlib

import jax
import jax.numpy as jnp
from jax import lax
from jax.sharding import PartitionSpec as P
from jax.experimental import pallas as pl
from jax.experimental.pallas import tpu as pltpu

RATE_SCALE = 8.0
NORM_EPS = 1e-06
SERIES_EDGE = 0.001
MESH = pl.DeviceIdType.MESH
SCOPES = False
OVER_ROWS = (((0,), (0,)), ((), ()))
OVER_COLS = (((1,), (1,)), ((), ()))


def scope(name):
    return jax.named_scope(name) if SCOPES else contextlib.nullcontext()


def partner_of(place, i, count):
    total = lax.rem(place + i, 2)
    bit = 2
    while bit < count:
        own = lax.div(place, bit) + lax.div(i, bit) + lax.div(i, 2 * bit)
        total = total + bit * lax.rem(own, 2)
        bit *= 2
    return total


def remote(src, dst, send_sem, recv_sem, device):
    return pltpu.make_async_remote_copy(
        src_ref=src,
        dst_ref=dst,
        send_sem=send_sem,
        recv_sem=recv_sem,
        device_id=device,
        device_id_type=MESH,
    )


def one_less_exp(spread):
    small = jnp.minimum(spread, 0.3)
    series = jnp.full_like(small, 1.0 / 40320.0)
    for factorial in (5040.0, 720.0, 120.0, 24.0, 6.0, 2.0, 1.0):
        series = 1.0 / factorial - small * series
    return jnp.where(spread < 0.3, small * series, 1.0 - jnp.exp(-spread))


def loop(begin, end, step):
    def body(i, carry):
        step(i)
        return carry

    lax.fori_loop(begin, end, body, 0)


def layer_kernel(
    sp_count,
    tp_count,
    refs_in,
    gate_grad,
    up_grad,
    down_grad,
    proj_grad,
    conv_grad,
    branch_grad,
    refs_here,
    maps,
    sending,
    moe_part,
    scaled_first,
    scaled_second,
    pre_values,
    held,
    part,
    from_beside,
    to_across,
    from_across,
    mine,
    leaving,
    arrived,
    full,
    hidden,
    d_gate,
    d_up,
    rate_factor,
    input_factor,
    direct_factor,
    gate_factor,
    gelu_values,
    keep,
    branch_all,
    mix,
    share,
    mix_all,
    small,
    small_all,
    load_sem,
    send_sem,
    recv_sem,
    back_send,
    back_recv,
    branch_send,
    branch_recv,
    last_send,
    last_recv,
    share_send,
    share_recv,
    small_send,
    small_recv,
):
    s = lax.axis_index("sp")
    t = lax.axis_index("tp")
    beside = t + 1 - 2 * lax.rem(t, 2)
    across = lax.rem(t + tp_count // 2, tp_count)
    facing = lax.rem(beside + tp_count // 2, tp_count)
    half = sp_count // 2
    s_twin = s + 1 - 2 * lax.rem(s, 2)
    (res, cot, gain, ids, weights, conv, gate, prev, decay, rate_map, input_map) = refs_here[:11]
    gate_w, up_w, down_w, proj = refs_here[11:]
    tok_rows, model_width = res.shape
    cap, width = sending.shape[2:]
    channels = conv.shape[1]
    share_rows, out_rows = share.shape[1:]

    def partner(i):
        return partner_of(s, i, sp_count)

    barrier = pltpu.get_barrier_semaphore()
    for other in (beside, across):
        pl.semaphore_signal(barrier, inc=1, device_id=(s, other), device_id_type=MESH)
    loop(
        1,
        sp_count,
        lambda i: pl.semaphore_signal(
            barrier, inc=1, device_id=(partner(i), t), device_id_type=MESH
        ),
    )
    loads = [
        pltpu.make_async_copy(src, dst, load_sem.at[k])
        for k, (src, dst) in enumerate(zip(refs_in, refs_here))
    ]
    for copy in loads:
        copy.start()
    for copy in loads[:5]:
        copy.wait()

    def cols_of(q):
        return pl.ds(pl.multiple_of(q * width, width), width)

    with scope("prepare"):
        cols = cols_of(t)
        res_all = res[...].astype(jnp.float32)
        inv_rms = lax.rsqrt(jnp.mean(res_all * res_all, axis=1, keepdims=True) + NORM_EPS)
        moe_part[...] = (res[:, cols].astype(jnp.float32) * inv_rms * gain[:, cols]).astype(
            jnp.bfloat16
        )
        square = (tok_rows, tok_rows)
        down_at = lax.broadcasted_iota(jnp.int32, square, 0)
        over_at = lax.broadcasted_iota(jnp.int32, square, 1)

        def column(row):
            return jnp.sum(jnp.where(down_at == over_at, row, 0.0), axis=1, keepdims=True)

        cot_mine = cot[:, cols].astype(jnp.float32)
        scaled_first[...] = (column(weights[0:1, :]) * cot_mine).astype(jnp.bfloat16)
        scaled_second[...] = (column(weights[1:2, :]) * cot_mine).astype(jnp.bfloat16)
        experts = lax.broadcasted_iota(jnp.int32, (sp_count, tok_rows), 0)
        is_first = ids[0:1, :] == experts
        is_second = ids[1:2, :] == experts
        hits = (is_first | is_second).astype(jnp.float32).astype(jnp.bfloat16)
        earlier = (down_at < over_at).astype(jnp.float32).astype(jnp.bfloat16)
        ranks = jnp.dot(hits, earlier, preferred_element_type=jnp.float32)
        row_first = jnp.sum(jnp.where(is_first, ranks, 0.0), axis=0, keepdims=True)
        row_second = jnp.sum(jnp.where(is_second, ranks, 0.0), axis=0, keepdims=True)
        row_first = row_first + (ids[0:1, :] * cap).astype(jnp.float32)
        row_second = row_second + (ids[1:2, :] * cap).astype(jnp.float32)
        slots = lax.broadcasted_iota(jnp.int32, (cap, tok_rows), 0).astype(jnp.float32)

    def filled(target):
        base = (target * cap).astype(jnp.float32)
        first = jnp.where(row_first - base == slots, 1.0, 0.0)
        second = jnp.where(row_second - base == slots, 1.0, 0.0)
        rows = jnp.dot(
            (first + second).astype(jnp.bfloat16),
            moe_part[...],
            preferred_element_type=jnp.float32,
        ).astype(jnp.bfloat16)
        from_first = jnp.dot(
            first.astype(jnp.bfloat16), scaled_first[...], preferred_element_type=jnp.float32
        )
        from_second = jnp.dot(
            second.astype(jnp.bfloat16), scaled_second[...], preferred_element_type=jnp.float32
        )
        return rows, (from_first + from_second).astype(jnp.bfloat16)

    def quarter_of(source, q):
        return held.at[source, :, :, cols_of(q)]

    def first(i):
        target = partner(i)
        return remote(
            sending.at[target], quarter_of(s, t), send_sem.at[0], recv_sem.at[0, i], (target, t)
        )

    def passed(kind, i, q, to):
        block = quarter_of(partner(i), q)
        landing = recv_sem.at[min(kind, 2), i]
        return remote(block, block, send_sem.at[kind], landing, (s, to))

    def landed(i):
        source = partner(i)
        remote(
            sending.at[source],
            quarter_of(source, t),
            send_sem.at[0],
            recv_sem.at[0, i],
            (source, t),
        ).wait_recv()

    def pass_on(i):
        passed(1, i, t, across).start()
        passed(2, i, t, beside).start()

    def pass_back(i):
        passed(1, i, across, across).wait_recv()
        passed(3, i, across, beside).start()

    def all_of(like, sem):
        return remote(like, like, sem, sem, (s, beside))

    def complete(i):
        all_of(sending.at[pl.ds(0, 2)], recv_sem.at[2, i]).wait_recv()

    rows_own, cot_own = filled(s)
    held[s, 0, :, cols] = rows_own
    held[s, 1, :, cols] = cot_own
    with scope("barrier"):
        pl.semaphore_wait(barrier, sp_count + 1)
    pass_on(0)

    def send_one(i):
        target = partner(i)
        rows, values = filled(target)
        sending[target, 0] = rows
        sending[target, 1] = values
        first(i).start()

    early = min(5, sp_count)
    with scope("sends"):
        loop(1, early, send_one)

    for copy in loads[5:11]:
        copy.wait()
    with scope("forward"):
        block = rate_map.shape[1]
        lane_in = lax.rem(lax.broadcasted_iota(jnp.int32, (block, channels), 1), block)
        spread_out = lane_in == lax.broadcasted_iota(jnp.int32, (block, channels), 0)
        spread_out = spread_out.astype(jnp.float32).astype(jnp.bfloat16)
        wide = (channels, channels)
        same = lax.div(lax.broadcasted_iota(jnp.int32, wide, 0), block) == lax.div(
            lax.broadcasted_iota(jnp.int32, wide, 1), block
        )
        for k, blocks in enumerate((rate_map, input_map)):
            tiled = jnp.dot(
                blocks[...].reshape(channels, block),
                spread_out,
                preferred_element_type=jnp.float32,
            )
            maps[:, k * channels : (k + 1) * channels] = jnp.where(same, tiled, 0.0).astype(
                jnp.bfloat16
            )
        pre_values[...] = jnp.dot(conv[...], maps[...], preferred_element_type=jnp.float32)
        y = jnp.exp(-decay[...])
        soft = y * (1.0 - y * (0.5 - y * (1.0 / 3.0 - y * (0.25 - y * 0.2))))
        step = 16

        def forward(i):
            rows = pl.ds(pl.multiple_of(i * step, step), step)
            rate_gate = jax.nn.sigmoid(pre_values[rows, :channels])
            input_gate = jax.nn.sigmoid(pre_values[rows, channels:])
            log_keep = -RATE_SCALE * rate_gate * soft
            kept = jnp.exp(log_keep)
            spread = -2.0 * log_keep
            gone = one_less_exp(spread)
            norm_term = jnp.sqrt(gone)
            conv_values = conv[rows, :].astype(jnp.float32)
            prev_values = prev[rows, :].astype(jnp.float32)
            inner = input_gate * conv_values
            state_now = kept * prev_values + norm_term * inner
            v = gate[rows, :].astype(jnp.float32)
            root = 0.7978845608028654
            bent = jnp.tanh(root * (v + 0.044715 * v * v * v))
            gelu_value = 0.5 * v * (1.0 + bent)
            gelu_slope = 0.5 * (1.0 + bent) + 0.5 * v * (1.0 - bent * bent) * root * (
                1.0 + 3.0 * 0.044715 * v * v
            )
            tiny_side = spread < SERIES_EDGE
            series = jnp.where(
                tiny_side, 1.0 + 0.5 * spread, spread / jnp.where(tiny_side, 1.0, gone)
            )
            slope = 0.5 * jnp.sqrt(spread * series)
            branch_all[s, rows, :] = (state_now * gelu_value).astype(jnp.bfloat16)
            rate_factor[rows, :] = prev_values * kept * (-RATE_SCALE * soft) * rate_gate * (
                1.0 - rate_gate
            ) + inner * kept * kept * (1.0 - rate_gate) * slope
            input_factor[rows, :] = norm_term * conv_values * input_gate * (1.0 - input_gate)
            direct_factor[rows, :] = norm_term * input_gate
            gate_factor[rows, :] = state_now * gelu_slope
            gelu_values[rows, :] = gelu_value
            keep[rows, :] = kept

        loop(0, tok_rows // step, forward)

    for copy in loads[11:]:
        copy.wait()

    def to_beside(i, k):
        source = partner(i)
        q = beside if k == 0 else facing
        return remote(
            part.at[source, :, cols_of(q)],
            from_beside.at[k, source],
            back_send.at[k],
            back_recv.at[k, i],
            (s, beside),
        )

    def crossing(i):
        source = partner(i)
        return remote(
            to_across.at[source],
            from_across.at[source],
            back_send.at[2],
            back_recv.at[2, i],
            (s, across),
        )

    def homeward(i):
        source = partner(i)
        return remote(
            leaving.at[source],
            arrived.at[s],
            back_send.at[3],
            back_recv.at[3, i],
            (source, t),
        )

    def expert(i):
        complete(i)
        source = partner(i)
        rows_in = held[source, 0]
        gate_pre = jnp.dot(rows_in, gate_w[...], preferred_element_type=jnp.float32)
        up_pre = jnp.dot(rows_in, up_w[...], preferred_element_type=jnp.float32)
        d_hidden = lax.dot_general(
            held[source, 1], down_w[...], OVER_COLS, preferred_element_type=jnp.float32
        )
        gate_sig = jax.nn.sigmoid(gate_pre)
        gate_act = gate_pre * gate_sig
        up_back = (d_hidden * gate_act).astype(jnp.bfloat16)
        gate_back = (d_hidden * up_pre * gate_sig * (1.0 + gate_pre * (1.0 - gate_sig))).astype(
            jnp.bfloat16
        )
        hidden[source] = (gate_act * up_pre).astype(jnp.bfloat16)
        d_up[source] = up_back
        d_gate[source] = gate_back
        back = lax.dot_general(
            gate_back, gate_w[...], OVER_COLS, preferred_element_type=jnp.float32
        )
        back = back + lax.dot_general(
            up_back, up_w[...], OVER_COLS, preferred_element_type=jnp.float32
        )
        part[source] = back.astype(jnp.bfloat16)
        to_beside(i, 1).start()
        to_beside(i, 0).start()

    def cross(i, at_once):
        to_beside(i, 1).wait_recv()
        at = partner(i)
        total = part[at, :, cols_of(across)].astype(jnp.float32) + from_beside[1, at].astype(
            jnp.float32
        )
        to_across[at] = total.astype(jnp.bfloat16)
        if at_once:
            crossing(i).start()
        to_beside(i, 0).wait_recv()
        mine[at] = part[at, :, cols].astype(jnp.float32) + from_beside[0, at].astype(jnp.float32)

    def leave(i):
        crossing(i).wait_recv()
        at = partner(i)
        total = (mine[at] + from_across[at].astype(jnp.float32)).astype(jnp.bfloat16)
        if isinstance(i, int) and i == 0:
            arrived[s] = total
        else:
            leaving[at] = total
            homeward(i).start()

    own_branch = branch_all.at[s]

    def branch_copy(j):
        return remote(
            own_branch,
            own_branch,
            branch_send.at[0],
            branch_recv.at[j],
            (partner(2 * j), t),
        )

    def branch_landed(j):
        source = partner(2 * j)
        return remote(
            own_branch,
            branch_all.at[source],
            branch_send.at[0],
            branch_recv.at[j],
            (source, t),
        )

    def branch_twin(j):
        block = branch_all.at[partner(2 * j)]
        return remote(block, block, branch_send.at[1], branch_recv.at[0], (s_twin, t))

    near = 4
    stride = 3 if sp_count == 8 else 2
    lag = 3 - stride

    def turn(i):
        @pl.when((i >= 2) & (i < sp_count + 2))
        def _():
            with scope("expert"):
                expert(i - 2)

        @pl.when((i >= near + 2) & (i < sp_count + 2))
        def _():
            with scope("cross"):
                cross(i - 2, True)

        @pl.when(i == sp_count)
        def _():
            crossing(3).start()

        @pl.when(i >= near + 3)
        def _():
            with scope("leave"):
                leave(i - 3)

        @pl.when(i == near + 3)
        def _():
            leave(0)
            leave(1)
            leave(2)

        @pl.when(i == sp_count + 1)
        def _():
            leave(3)

        @pl.when((i >= 1) & (i < sp_count))
        def _():
            with scope("landed"):
                landed(i)
            pass_on(i)

        @pl.when(i == 1)
        def _():
            branch_twin(0).start()

        @pl.when((i >= 3) & (i <= stride * (half - 2) + lag) & (lax.rem(i - lag, stride) == 0))
        def _():
            branch_copy(lax.div(i - lag, stride)).start()

        @pl.when((i >= 1) & (i + early - 1 < sp_count))
        def _():
            send_one(i + early - 1)

        @pl.when(i == near + 1)
        def _():
            crossing(0).start()
            crossing(1).start()
            crossing(2).start()

        @pl.when((i >= 1) & (i < sp_count + 1))
        def _():
            with scope("pass_back"):
                pass_back(i - 1)

        @pl.when((i >= 2) & (i < near + 2))
        def _():
            with scope("cross"):
                cross(i - 2, False)

    loop(0, sp_count + 3, turn)

    def pass_branch(j):
        branch_landed(j).wait_recv()
        branch_twin(j).start()

    with scope("branch_pass"):
        loop(1, half - 1, pass_branch)

    def merged(values):
        return values.reshape(sp_count * cap, values.shape[2])

    def summed(left, right):
        if cap % 16 == 0:
            return lax.dot_general(
                merged(left), merged(right), OVER_ROWS, preferred_element_type=jnp.float32
            )
        total = None
        for source in range(sp_count):
            one = lax.dot_general(
                left[source], right[source], OVER_ROWS, preferred_element_type=jnp.float32
            )
            total = one if total is None else total + one
        return total

    tile = 256
    def rows_tile(k):
        at = pl.ds(pl.multiple_of(k * tile, tile), tile)
        rows = held[:, 0, :, at]
        gate_grad[at, :] = summed(rows, d_gate[...])
        up_grad[at, :] = summed(rows, d_up[...])

    def cot_tile(k):
        at = pl.ds(pl.multiple_of(k * tile, tile), tile)
        down_grad[:, at] = summed(hidden[...], held[:, 1, :, at])

    with scope("grads_rows"):
        loop(0, model_width // tile, rows_tile)

    lanes = lax.broadcasted_iota(jnp.int32, (tok_rows, cap), 1).astype(jnp.float32)
    slot_first, slot_second = column(row_first), column(row_second)

    def gather_rows(source):
        base = (source * cap).astype(jnp.float32)
        chosen = jnp.where(slot_first - base == lanes, 1.0, 0.0)
        chosen = chosen + jnp.where(slot_second - base == lanes, 1.0, 0.0)
        return jnp.dot(
            chosen.astype(jnp.bfloat16), arrived[source], preferred_element_type=jnp.float32
        )

    def add_in(i, total):
        source = partner(i)
        with scope("home"):
            remote(
                leaving.at[source],
                arrived.at[source],
                back_send.at[3],
                back_recv.at[3, i],
                (source, t),
            ).wait_recv()
        return total + gather_rows(source)

    full[:, cols] = lax.fori_loop(1, sp_count, add_in, gather_rows(s)).astype(jnp.bfloat16)

    pair, other_pair = lax.div(t, 2), lax.div(across, 2)

    def rows_of(q):
        return pl.ds(pl.multiple_of(q * share_rows, share_rows), share_rows)

    def pair_rows(p):
        return pl.ds(pl.multiple_of(p * 2 * share_rows, 2 * share_rows), 2 * share_rows)

    def given(kind, rows, q, to):
        block = full.at[rows, cols_of(q)]
        return remote(block, block, last_send.at[kind], last_recv.at[kind], (s, to))

    def own_first(kind, mine_too):
        peer = (across, beside, facing)[kind]
        return given(kind, rows_of(t), peer, peer) if mine_too else given(kind, rows_of(peer), t, peer)

    for kind in (2, 0, 1):
        own_first(kind, False).start()

    def rest_across(at_peer):
        if at_peer:
            return (
                given(3, pair_rows(other_pair), across, across),
                given(4, rows_of(beside), across, across),
            )
        return given(3, pair_rows(pair), t, across), given(4, rows_of(facing), t, across)

    def rest_beside(at_peer):
        if at_peer:
            return (
                given(5, pair_rows(other_pair), beside, beside),
                given(6, rows_of(beside), beside, beside),
            )
        return given(5, pair_rows(other_pair), t, beside), given(6, rows_of(t), t, beside)

    def rest_facing(at_peer):
        if at_peer:
            return (
                given(7, pair_rows(other_pair), facing, beside),
                given(8, rows_of(beside), facing, beside),
            )
        return given(7, pair_rows(other_pair), across, beside), given(8, rows_of(t), across, beside)

    for copy in rest_across(False) + rest_beside(False):
        copy.start()
    branch_copy(half - 1).start()
    with scope("grads_cot"):
        loop(0, model_width // tile, cot_tile)
    with scope("quarter"):
        for kind in range(3):
            own_first(kind, True).wait_recv()

    def mix_rows(begin):
        rows = pl.ds(pl.multiple_of(begin, share_rows), share_rows)
        values = res[rows, :].astype(jnp.float32)
        weighted = gain[...] * full[rows, :].astype(jnp.float32)
        inverse = lax.rsqrt(jnp.mean(values * values, axis=1, keepdims=True) + NORM_EPS)
        cubed = inverse * inverse * inverse
        slope = cubed * jnp.mean(values * weighted, axis=1, keepdims=True)
        return rows, (
            cot[rows, :].astype(jnp.float32) + inverse * weighted - values * slope
        ).astype(jnp.bfloat16)

    def share_view(source, q):
        return mix_all.at[source, pl.ds(pl.multiple_of(q * share_rows, share_rows), share_rows), :]

    def share_first(i):
        target = partner(i)
        return remote(
            share.at[target],
            share_view(s, t),
            share_send.at[0],
            share_recv.at[0, i],
            (target, t),
        )

    def share_passed(kind, i, q, to):
        block = share_view(partner(i), q)
        landing = share_recv.at[1, i] if kind == 1 else share_recv.at[0, 0]
        return remote(block, block, share_send.at[kind], landing, (s, to))

    def share_landed(i):
        source = partner(i)
        remote(
            share.at[source],
            share_view(source, t),
            share_send.at[0],
            share_recv.at[0, i],
            (source, t),
        ).wait_recv()

    straight = 5 * sp_count // 8

    def share_on(i):
        share_passed(1, i, t, across).start()

        @pl.when(i >= straight)
        def _():
            share_passed(3, i, t, facing).start()

        share_passed(2, i, t, beside).start()

    def share_back(i):
        share_passed(1, i, across, across).wait_recv()

        @pl.when(i < straight)
        def _():
            share_passed(3, i, across, beside).start()

    with scope("share"):
        _, own_rows = mix_rows(t * share_rows)
        for j in range(sp_count):
            share[j] = own_rows[:, j * out_rows : (j + 1) * out_rows]
        loop(1, sp_count, lambda i: share_first(sp_count - i).start())
        own_at = pl.ds(pl.multiple_of(t * share_rows, share_rows), share_rows)
        mix_all[s, own_at, :] = share[s]
        share_on(0)

    with scope("quarter_late"):
        for copy in rest_across(True):
            copy.wait_recv()
        for copy in rest_facing(False):
            copy.start()
        for copy in rest_beside(True) + rest_facing(True):
            copy.wait_recv()

    def relay(i):
        share_landed(i)
        share_on(i)

    with scope("relay"):
        loop(1, sp_count, relay)

    with scope("mix"):

        def fill(k):
            rows, values = mix_rows(k * share_rows)
            mix[rows, :] = values

        loop(0, tp_count, fill)

    with scope("scan"):
        d_branch = jnp.dot(mix[...], proj[...], preferred_element_type=jnp.float32)
        branch_grad[...] = d_branch * gate_factor[...]
        at = lax.broadcasted_iota(jnp.int32, d_branch.shape, 0)
        grads = d_branch * gelu_values[...]
        keeps = jnp.where(at < tok_rows - 1, pltpu.roll(keep[...], tok_rows - 1, 0), 1.0)
        reach = 1
        while reach < tok_rows:
            inside = at < tok_rows - reach
            later_grads = jnp.where(inside, pltpu.roll(grads, tok_rows - reach, 0), 0.0)
            later_keeps = jnp.where(inside, pltpu.roll(keeps, tok_rows - reach, 0), 1.0)
            grads = grads + keeps * later_grads
            keeps = keeps * later_keeps
            reach *= 2
        small[...] = jnp.zeros_like(small)
        small[0:1, :] = keep[0:1, :] * keeps[0:1, :]
        small[1:2, :] = keep[0:1, :] * grads[0:1, :]
        small_all[s] = jnp.zeros(small.shape, jnp.float32)

    def carry_to(i):
        return remote(
            small, small_all.at[s], small_send.at[0], small_recv.at[0], (partner(i), t)
        )

    loop(1, sp_count, lambda i: carry_to(i).start())

    with scope("branch_last"):
        pass_branch(half - 1)

    with scope("relay_back"):
        loop(0, sp_count, share_back)

    with scope("small"):
        all_of(small_all.at[pl.ds(0, sp_count - 1)], small_recv.at[0]).wait_recv()

    def compose(turn, carried):
        source = sp_count - 1 - turn
        later = small_all[source]
        return jnp.where(source > s, later[1:2] + later[0:1] * carried, carried)

    with scope("back_maps"):
        carried = lax.fori_loop(0, sp_count - 1, compose, jnp.zeros((1, channels), jnp.float32))
        state_grad = grads + keeps * carried
        back = jnp.concatenate(
            [state_grad * rate_factor[...], state_grad * input_factor[...]], axis=1
        )
        high = back.astype(jnp.bfloat16)
        low = (back - high.astype(jnp.float32)).astype(jnp.bfloat16)
        conv_grad[...] = (
            state_grad * direct_factor[...]
            + lax.dot_general(high, maps[...], OVER_COLS, preferred_element_type=jnp.float32)
            + lax.dot_general(low, maps[...], OVER_COLS, preferred_element_type=jnp.float32)
        )

    with scope("last_waits"):

        all_of(mix_all.at[:, pl.ds(0, 2 * share_rows)], share_recv.at[0, 0]).wait_recv()
        all_of(branch_all.at[pl.ds(0, half)], branch_recv.at[0]).wait_recv()
    with scope("grad_proj"):
        proj_grad[...] = lax.dot_general(
            mix_all[...].reshape(sp_count * tok_rows, out_rows),
            branch_all[...].reshape(sp_count * tok_rows, channels),
            OVER_ROWS,
            preferred_element_type=jnp.float32,
        )

    others = pl.ds(0, sp_count - 1)
    with scope("end"):
        all_of(sending.at[others], send_sem.at[0]).wait_send()
        for kind in (1, 2, 3):
            all_of(sending, send_sem.at[kind]).wait_send()
            all_of(to_across, back_send.at[kind - 1]).wait_send()
            all_of(share, share_send.at[kind]).wait_send()
        all_of(to_across.at[others], back_send.at[3]).wait_send()
        all_of(share.at[others], share_send.at[0]).wait_send()
        all_of(small_all.at[others], small_send.at[0]).wait_send()
        all_of(branch_all.at[pl.ds(0, half - 1)], branch_send.at[0]).wait_send()
        all_of(branch_all.at[pl.ds(0, half)], branch_send.at[1]).wait_send()
        for kind in range(3):
            own_first(kind, False).wait_send()
        for copy in rest_across(False) + rest_beside(False) + rest_facing(False):
            copy.wait_send()


def layer(sp_count, tp_count, cap, operands):
    res, conv, gate_w, down_w = (operands[k] for k in (0, 5, 11, 13))
    tok_rows, model_width = res.shape
    channels, units = conv.shape[1], down_w.shape[0]
    width = model_width // tp_count
    share_rows, out_rows = tok_rows // tp_count, model_width // sp_count
    vmem = pl.BlockSpec(memory_space=pltpu.VMEM)
    anywhere = pl.BlockSpec(memory_space=pl.ANY)
    low, exact = jnp.bfloat16, jnp.float32
    blocks = (sp_count, cap, width)
    scratch = [
        ((channels, 2 * channels), low),
        ((sp_count, 2, cap, width), low),
        ((tok_rows, width), low),
        ((tok_rows, width), low),
        ((tok_rows, width), low),
        ((tok_rows, 2 * channels), exact),
        ((sp_count, 2, cap, model_width), low),
        ((sp_count, cap, model_width), low),
        ((2,) + blocks, low),
        (blocks, low),
        (blocks, low),
        (blocks, exact),
        (blocks, low),
        (blocks, low),
        (res.shape, low),
        ((sp_count, cap, units), low),
        ((sp_count, cap, units), low),
        ((sp_count, cap, units), low),
    ]
    scratch += [(conv.shape, exact)] * 6
    scratch += [
        ((sp_count,) + conv.shape, low),
        (res.shape, low),
        ((sp_count, share_rows, out_rows), low),
        ((sp_count, tok_rows, out_rows), low),
        ((8, channels), exact),
        ((sp_count, 8, channels), exact),
    ]
    sems = [
        (len(operands),),
        (4,),
        (3, sp_count),
        (4,),
        (4, sp_count),
        (2,),
        (sp_count // 2,),
        (9,),
        (9,),
        (4,),
        (2, sp_count),
        (1,),
        (1,),
    ]
    def grouped(*refs):
        layer_kernel(sp_count, tp_count, refs[: len(operands)], *refs[len(operands) :])

    return pl.pallas_call(
        grouped,
        out_shape=[
            pltpu.VMEM(shape, exact)
            for shape in (
                gate_w.shape,
                gate_w.shape,
                down_w.shape,
                (out_rows, channels),
                conv.shape,
                conv.shape,
            )
        ],
        in_specs=[anywhere] * len(operands),
        out_specs=[vmem] * 6,
        scratch_shapes=[[pltpu.VMEM(given.shape, given.dtype) for given in operands]]
        + [pltpu.VMEM(shape, kind) for shape, kind in scratch]
        + [pltpu.SemaphoreType.DMA(shape) for shape in sems],
        compiler_params=pltpu.CompilerParams(collective_id=1, has_side_effects=True, vmem_limit_bytes=59_000_000),
        cost_estimate=pl.CostEstimate(flops=0, bytes_accessed=40_000_000, transcendentals=0),
    )(*operands)


def store_kernel(*refs):
    count = len(refs) // 2
    sems = refs[-1]
    copies = [
        pltpu.make_async_copy(refs[k], refs[count + k], sems.at[k]) for k in range(count)
    ]
    for copy in copies:
        copy.start()
    for copy in copies:
        copy.wait()


def store(values):
    return pl.pallas_call(
        store_kernel,
        out_shape=[jax.ShapeDtypeStruct(value.shape, value.dtype) for value in values],
        in_specs=[pl.BlockSpec(memory_space=pltpu.VMEM)] * len(values),
        out_specs=[pl.BlockSpec(memory_space=pl.ANY)] * len(values),
        scratch_shapes=[pltpu.SemaphoreType.DMA((len(values),))],
        compiler_params=pltpu.CompilerParams(vmem_limit_bytes=16 * 1024 * 1024),
    )(*[pltpu.with_memory_space_constraint(value, pltpu.VMEM) for value in values])


def per_device(
    cotangent,
    residual,
    norm_gain,
    route_ids,
    route_weights,
    expert_gate,
    expert_up,
    expert_down,
    out_proj,
    conv_out,
    branch_gate,
    prev_state,
    decay_param,
    rate_map,
    input_map,
):
    sp_count = lax.axis_size("sp")
    tp_count = lax.axis_size("tp")
    experts_all = expert_gate.shape[0] * sp_count
    capacity = 4 * residual.shape[0] // experts_all
    grads = layer(
        sp_count,
        tp_count,
        capacity,
        (
            residual,
            cotangent,
            norm_gain[None, :],
            route_ids.T,
            route_weights.T,
            conv_out,
            branch_gate,
            prev_state,
            decay_param[None, :],
            rate_map,
            input_map,
            expert_gate[0],
            expert_up[0],
            expert_down[0],
            out_proj,
        ),
    )
    grad_gate, grad_up, grad_down, grad_out_proj, grad_conv_out, grad_branch_gate = store(grads)
    return (
        grad_gate[None],
        grad_up[None],
        grad_down[None],
        grad_out_proj,
        grad_conv_out,
        grad_branch_gate,
    )


def solution(mesh):
    in_specs = (
        P("sp", None),
        P("sp", None),
        P(),
        P("sp", None),
        P("sp", None),
        P("sp", None, "tp"),
        P("sp", None, "tp"),
        P("sp", "tp", None),
        P(None, "tp"),
        P("sp", "tp"),
        P("sp", "tp"),
        P("sp", "tp"),
        P("tp"),
        P("tp", None, None),
        P("tp", None, None),
    )
    out_specs = (
        P("sp", None, "tp"),
        P("sp", None, "tp"),
        P("sp", "tp", None),
        P("sp", "tp"),
        P("sp", "tp"),
        P("sp", "tp"),
    )
    return jax.shard_map(
        per_device, mesh=mesh, in_specs=in_specs, out_specs=out_specs, check_vma=False
    )
```
